32 devices in a mesh: sp: 8 (over z, y), tp: 4 (over x, core).
Axes of the slice: x: 2, y: 2, z: 4, core: 2. Of those that a mesh axis runs over, the one named last changes fastest.
Arguments:
- residual: bfloat16 [8192, 2048], P(('sp', 'tp')), may hold values from -6 to 6
- pool_input: bfloat16 [8192, 1024], P('sp', 'tp'), may hold values from -6 to 6
- doc_ids: int32 [8192], P('sp'), may hold values from 0 to 3, never falling along the last dimension, each value on 1 to 4096 neighbouring positions
- pool_map: bfloat16 [4, 256, 256], P('tp'), may hold values from -0.375 to 0.375
- pool_scale: float32 [1024], P('tp'), may hold values from 0.1 to 1.9
- out_weight: bfloat16 [1024, 2048], replicated, may hold values from -0.1875 to 0.1875
- mix_gain: float32 [2048], replicated, may hold values from 0.1 to 1.9
- mix_shift: float32 [2048], replicated, may hold values from -1.75 to 1.75
- group_router: bfloat16 [2048, 4], replicated, may hold values from -0.125 to 0.125
- expert_router: bfloat16 [2048, 8], replicated, may hold values from -0.125 to 0.125
- expert_gate: bfloat16 [8, 2048, 512], P('sp'), may hold values from -0.375 to 0.375
- expert_up: bfloat16 [8, 2048, 512], P('sp'), may hold values from -0.375 to 0.375
- expert_down: bfloat16 [8, 512, 2048], P('sp'), may hold values from -0.75 to 0.75
- routes: int32 [8192, 2], P(('sp', 'tp')), may hold values from 0 to 7, as said below
- ffn_gain: float32 [2048], replicated, may hold values from 0.1 to 1.9
- ffn_shift: float32 [2048], replicated, may hold values from -1.75 to 1.75
Outputs:
- layer_out: bfloat16 [8192, 2048], P(('sp', 'tp'))
The draws below stay inside these ranges and needn't reach their ends.
Inputs may be any that keep to these rules, and one draw needn't show every extreme that they name: `doc_ids`: document numbers never fall along the positions; each document has 1 to 4096 positions. `routes`: A token names 2 different experts. In each aligned block of half of one device's 256 rows, 4 experts are named exactly 64 times each and the others not at all.
All inputs are finite; a program needn't handle non-finite values.
Results may differ from the reference program's by a relative error of at most 0.0073.
Values may be sent and summed in bfloat16 or wider, within the bound.
A program may use at most 128 MiB of HBM per device.

```python
import math
import jax
import jax.numpy as jnp
import numpy as np
from jax import lax

D = 2048
POOL = 1024
PGROUPS = 4
GW = 256
FF = 512
MGROUPS = 4
TOPK = 2
SEQ_DEV = 1024
ROWS = 256
TOKENS = 8192
EXPERTS = 8
SLOTS = 64
N_SP = 8


def draw_routes(key, part):
    block_rows = ROWS // 2
    block_count = TOKENS // block_rows
    named_count = EXPERTS // 2
    anchor = jax.random.randint(jax.random.fold_in(key, 7), (), 0, EXPERTS).astype(jnp.int32)
    block_seeds = jax.random.split(jax.random.fold_in(key, 11), block_count)

    def one_block(block_seed):
        seeds = jax.random.split(block_seed, TOPK + 2)
        others = (anchor + 1 + jax.random.permutation(seeds[0], EXPERTS - 1).astype(jnp.int32)) % EXPERTS
        chosen = jnp.concatenate([anchor[None], others[:named_count - 1]]).astype(jnp.int32)
        listed = chosen[jnp.arange(named_count * SLOTS, dtype=jnp.int32) // SLOTS]
        columns = []
        for column in range(TOPK):
            segment = listed[column * block_rows:(column + 1) * block_rows]
            order = jax.random.permutation(seeds[column + 1], block_rows).astype(jnp.int32)
            columns.append(segment[order])
        table = jnp.stack(columns, axis=1)
        rotation = jax.random.randint(seeds[TOPK + 1], (block_rows,), 0, TOPK).astype(jnp.int32)
        column_index = (jnp.arange(TOPK, dtype=jnp.int32)[None, :] + rotation[:, None]) % TOPK
        return jnp.take_along_axis(table, column_index, axis=1)
    blocks = jax.vmap(one_block)(block_seeds)
    return blocks.reshape(TOKENS, TOPK).astype(jnp.int32)


def level_of(stream_key, shape, shards, low, high):
    level, own = 1.0, jax.random.fold_in(stream_key, 6)
    for position, shards_of in shards:
        steps = jnp.exp(jax.random.uniform(jax.random.fold_in(own, position), (shards_of,), jnp.float32, low / len(shards), high / len(shards)))
        level = level * jnp.repeat(steps, shape[position] // shards_of).reshape([-1 if axis == position else 1 for axis in range(len(shape))])
    return level


def length_profile(amount, total, bound, lean):
    portions = [(1 << 20) // math.isqrt(rank ** lean) + 1 for rank in range(2, amount + 1)]
    spare, given = total - bound - (amount - 1), [1] * (amount - 1)
    while spare > 0:
        free = [i for i in range(amount - 1) if given[i] < bound]
        pool, remaining = sum([portions[i] for i in free]), spare
        for i in free:
            extra = min(bound - given[i], max(1, remaining * portions[i] // pool), spare)
            given[i] = given[i] + extra
            spare = spare - extra
    return np.array([bound] + given)


def uneven(stream_key, number_of, total, limit, slope):
    if number_of == 2:
        one = jax.random.randint(stream_key, (), max(1, total - limit), min(limit, total - 1) + 1)
        return jnp.stack([one, total - one])
    tallies = jnp.asarray(length_profile(number_of, total, limit, slope), jnp.int32)
    couples = (number_of - 1) // 2
    source_of, taker = tallies[1:1 + 2 * couples:2], tallies[2:2 + 2 * couples:2]
    slack = jnp.minimum(source_of - 1, limit - taker)
    moved = jax.random.randint(jax.random.fold_in(stream_key, 1), (couples,), 0, 1 << 20) % (slack + 1)
    tallies = tallies.at[1:1 + 2 * couples:2].set(source_of - moved).at[2:2 + 2 * couples:2].set(taker + moved)
    return tallies[jax.random.permutation(jax.random.fold_in(stream_key, 2), number_of)]


def bell_draw(rng, dims, width, reach, cuts=(), kind=jnp.bfloat16):
    values = jax.random.normal(rng, dims, jnp.float32) * width
    if len(cuts) > 0:
        values = level_of(rng, dims, cuts, -0.22, 0.18) * values
    return jnp.clip(values, min=-reach, max=reach).astype(kind)


def setup_inputs(seed: int = 0) -> dict:
    key_list = jax.random.split(jax.random.key(seed), 17)
    residual = bell_draw(key_list[0], (TOKENS, D), 1.0, 6.0, ((0, 32),))
    pool_input = bell_draw(key_list[1], (TOKENS, POOL), 1.0, 6.0, ((0, 8), (1, 4)))
    doc_ids = jnp.searchsorted(jnp.cumsum(uneven(key_list[2], N_SP // 2, TOKENS, 4 * SEQ_DEV, 1)), jnp.arange(TOKENS), side="right").astype(jnp.int32)
    pool_map = bell_draw(key_list[3], (PGROUPS, GW, GW), GW ** -0.5, 0.375, ((0, 4),))
    pool_scale = jnp.clip(1.0 + 0.18 * jax.random.normal(key_list[4], (POOL,), jnp.float32), 0.1, 1.9)
    out_weight = bell_draw(key_list[5], (POOL, D), POOL ** -0.5, 0.1875)
    mix_gain = jnp.clip(1.0 + 0.18 * jax.random.normal(key_list[6], (D,), jnp.float32), 0.1, 1.9)
    mix_shift = bell_draw(key_list[7], (D,), 0.3, 1.75, (), jnp.float32)
    group_router = bell_draw(key_list[8], (D, MGROUPS), D ** -0.5, 0.125)
    expert_router = bell_draw(key_list[9], (D, EXPERTS), D ** -0.5, 0.125)
    expert_gate = bell_draw(key_list[10], (EXPERTS, D, FF), (D // 8) ** -0.5, 0.375, ((0, 8),))
    expert_up = bell_draw(key_list[11], (EXPERTS, D, FF), (D // 8) ** -0.5, 0.375, ((0, 8),))
    expert_down = bell_draw(key_list[12], (EXPERTS, FF, D), (FF // 8) ** -0.5, 0.75, ((0, 8),))
    routes = draw_routes(jax.random.fold_in(key_list[16], 71), 0)
    ffn_gain = jnp.clip(1.0 + 0.18 * jax.random.normal(key_list[14], (D,), jnp.float32), 0.1, 1.9)
    ffn_shift = bell_draw(key_list[15], (D,), 0.3, 1.75, (), jnp.float32)
    return {"residual": residual, "pool_input": pool_input, "doc_ids": doc_ids, "pool_map": pool_map, "pool_scale": pool_scale, "out_weight": out_weight, "mix_gain": mix_gain, "mix_shift": mix_shift, "group_router": group_router, "expert_router": expert_router, "expert_gate": expert_gate, "expert_up": expert_up, "expert_down": expert_down, "routes": routes, "ffn_gain": ffn_gain, "ffn_shift": ffn_shift}


skip_scale = 2.0 ** 0.5
epsilon = 1e-05

def layer_norm(values, norm_gain, norm_shift):
    center = values - lax.optimization_barrier(jnp.mean(values, axis=-1, keepdims=True))
    spread = lax.optimization_barrier(jnp.mean(center * center, axis=-1, keepdims=True))
    return center * lax.rsqrt(spread + epsilon) * norm_gain + norm_shift

def route_weights(normed, chosen, group_router, expert_router):
    group_logits = jnp.dot(normed, group_router, preferred_element_type=jnp.float32)
    expert_logits = jnp.dot(normed, expert_router, preferred_element_type=jnp.float32)
    group_count = group_logits.shape[1]
    expert_count = expert_logits.shape[1]
    group_exp = jnp.exp(group_logits)
    group_prob = group_exp / lax.optimization_barrier(jnp.sum(group_exp, axis=1, keepdims=True))
    expert_ids = jnp.arange(expert_count, dtype=jnp.int32)
    picked = lax.optimization_barrier(jnp.sum(jnp.where(chosen[:, :, None] == expert_ids[None, None, :], expert_logits[:, None, :], 0.0), axis=2))
    picked_exp = jnp.exp(picked)
    pair_share = picked_exp / lax.optimization_barrier(jnp.sum(picked_exp, axis=1, keepdims=True))
    group_of = chosen // (expert_count // group_count)
    group_ids = jnp.arange(group_count, dtype=jnp.int32)
    group_share = lax.optimization_barrier(jnp.sum(jnp.where(group_of[:, :, None] == group_ids[None, None, :], group_prob[:, None, :], 0.0), axis=2))
    return group_share * pair_share

def pool_group(values, doc_ids, window):
    length = values.shape[0]
    source = values.astype(jnp.float32)
    running = jnp.zeros_like(source)
    weight_sum = jnp.zeros((length, 1), jnp.float32)
    for offset in range(window):
        earlier = jnp.pad(source, ((offset, 0), (0, 0)))[:length]
        earlier_docs = jnp.pad(doc_ids, (offset, 0), constant_values=-1)[:length]
        same_doc = (earlier_docs == doc_ids).astype(jnp.float32)[:, None]
        running = running + same_doc * earlier
        weight_sum = weight_sum + same_doc
    return running / weight_sum - source

def expert_sum(normed, routes, weight, expert_gate, expert_up, expert_down):
    flat_routes = routes.reshape(-1).astype(jnp.int32)
    entry_count = flat_routes.shape[0]
    sorted_entries = jnp.argsort(flat_routes, stable=True).astype(jnp.int32)
    counts = lax.optimization_barrier(jnp.sum((flat_routes[:, None] == jnp.arange(EXPERTS, dtype=jnp.int32)[None, :]).astype(jnp.int32), axis=0))
    starts = (jnp.cumsum(counts) - counts).astype(jnp.int32)
    load_limit = TOKENS // (ROWS // 2) * SLOTS
    entries_padded = jnp.concatenate([sorted_entries, jnp.full((load_limit,), entry_count, jnp.int32)])
    flat_weight = jnp.concatenate([weight.reshape(-1), jnp.zeros((1,), jnp.float32)])
    padded_rows = jnp.concatenate([normed, jnp.zeros((1, normed.shape[1]), normed.dtype)], axis=0)

    def expert_step(routed_sum, expert):
        entry_ids = lax.dynamic_slice_in_dim(entries_padded, starts[expert], load_limit)
        live_mask = jnp.arange(load_limit, dtype=jnp.int32) < counts[expert]
        entry_ids = jnp.where(live_mask, entry_ids, entry_count).astype(jnp.int32)
        token_ids = (entry_ids // TOPK).astype(jnp.int32)
        gathered = padded_rows[token_ids]
        gate_out = jnp.dot(gathered, expert_gate[expert], preferred_element_type=jnp.float32)
        up_out = jnp.dot(gathered, expert_up[expert], preferred_element_type=jnp.float32)
        hidden = (jax.nn.silu(gate_out) * up_out).astype(jnp.bfloat16)
        result = jnp.dot(hidden, expert_down[expert], preferred_element_type=jnp.float32).astype(jnp.bfloat16)
        term = flat_weight[entry_ids][:, None] * result.astype(jnp.float32)
        return (routed_sum.at[token_ids].add(term), None)
    routed_sum = jnp.zeros((TOKENS + 1, normed.shape[1]), jnp.float32)
    routed_sum, unused = lax.scan(expert_step, routed_sum, jnp.arange(EXPERTS, dtype=jnp.int32))
    return routed_sum[:TOKENS]

def reference(residual, pool_input, doc_ids, pool_map, pool_scale, out_weight, mix_gain, mix_shift, group_router, expert_router, expert_gate, expert_up, expert_down, routes, ffn_gain, ffn_shift):
    mixed_parts = []
    for group_index in range(PGROUPS):
        columns = slice(group_index * GW, (group_index + 1) * GW)
        pooled = pool_group(pool_input[:, columns], doc_ids, 2 ** (group_index + 1)).astype(jnp.bfloat16)
        mapped = jnp.dot(pooled, pool_map[group_index], preferred_element_type=jnp.float32) * pool_scale[columns]
        mixed_parts.append(mapped.astype(jnp.bfloat16))
    mixed = jnp.concatenate(mixed_parts, axis=1)
    branch = jnp.dot(mixed, out_weight, preferred_element_type=jnp.float32)
    normed = layer_norm(skip_scale * residual.astype(jnp.float32) + branch, mix_gain, mix_shift).astype(jnp.bfloat16)
    weight = route_weights(normed, routes, group_router, expert_router)
    routed = expert_sum(normed, routes, weight, expert_gate, expert_up, expert_down)
    return layer_norm(skip_scale * normed.astype(jnp.float32) + routed, ffn_gain, ffn_shift).astype(jnp.bfloat16)
```

```python
import functools

import jax
import jax.numpy as jnp
from jax import lax
from jax.experimental import pallas as pl
from jax.experimental.pallas import tpu as pltpu
from jax.sharding import PartitionSpec as P

skip_scale = 2.0**0.5
epsilon = 1e-05


def from_behind(block, axis, distance):
    devices = range(lax.axis_size(axis))
    route = [(i - distance, i) for i in devices if i - distance in devices]
    return lax.ppermute(block, axis, route)


def layer_norm(values, norm_gain, norm_shift):
    center = values - jnp.mean(values, axis=-1, keepdims=True)
    spread = jnp.mean(center * center, axis=-1, keepdims=True)
    return center * lax.rsqrt(spread + epsilon) * norm_gain + norm_shift


def route_weights(normed, chosen, group_router, expert_router):
    group_logits = jnp.dot(normed, group_router, preferred_element_type=jnp.float32)
    expert_logits = jnp.dot(normed, expert_router, preferred_element_type=jnp.float32)
    group_count = group_logits.shape[1]
    expert_count = expert_logits.shape[1]
    group_exp = jnp.exp(group_logits)
    group_prob = group_exp / jnp.sum(group_exp, axis=1, keepdims=True)
    expert_ids = jnp.arange(expert_count, dtype=jnp.int32)
    picked = jnp.sum(
        jnp.where(chosen[:, :, None] == expert_ids[None, None, :], expert_logits[:, None, :], 0.0),
        axis=2,
    )
    picked_exp = jnp.exp(picked)
    pair_share = picked_exp / jnp.sum(picked_exp, axis=1, keepdims=True)
    group_of = chosen // (expert_count // group_count)
    group_ids = jnp.arange(group_count, dtype=jnp.int32)
    group_share = jnp.sum(
        jnp.where(group_of[:, :, None] == group_ids[None, None, :], group_prob[:, None, :], 0.0),
        axis=2,
    )
    return group_share * pair_share


def expert_ffn(arrived, expert_gate, expert_up, expert_down):
    sources, slot_count, width = arrived.shape
    gathered = arrived.reshape(sources * slot_count, width)
    gate_out = jnp.dot(gathered, expert_gate[0], preferred_element_type=jnp.float32)
    up_out = jnp.dot(gathered, expert_up[0], preferred_element_type=jnp.float32)
    hidden = (jax.nn.silu(gate_out) * up_out).astype(jnp.bfloat16)
    result = jnp.dot(hidden, expert_down[0], preferred_element_type=jnp.float32).astype(
        jnp.bfloat16
    )
    return result.reshape(sources, slot_count, width)


def fill_slots(normed, chosen, capacity, expert_count):
    flat_routes = chosen.reshape(-1)
    entry_count = flat_routes.shape[0]
    onehot = (flat_routes[:, None] == jnp.arange(expert_count, dtype=jnp.int32)[None, :]).astype(
        jnp.int32
    )
    slot_rank = jnp.sum((jnp.cumsum(onehot, axis=0) - onehot) * onehot, axis=1)
    slot_index = flat_routes * capacity + slot_rank
    token_ids = jnp.arange(entry_count, dtype=jnp.int32) // chosen.shape[1]
    source_row = (
        jnp.full((expert_count * capacity,), normed.shape[0], jnp.int32)
        .at[slot_index]
        .set(token_ids)
    )
    padded = jnp.concatenate([normed, jnp.zeros((1, normed.shape[1]), normed.dtype)], axis=0)
    outgoing = jnp.take(padded, source_row, axis=0).reshape(expert_count, capacity, normed.shape[1])
    return (outgoing, slot_index)


def combine_rows(returned, slot_index, weight):
    flat_out = returned.reshape(-1, returned.shape[2])
    picked = jnp.take(flat_out, slot_index, axis=0).reshape(
        weight.shape[0], weight.shape[1], flat_out.shape[1]
    )
    return jnp.sum(weight[:, :, None] * picked.astype(jnp.float32), axis=1)


MESH = pl.DeviceIdType.MESH
group_size = 4
block = 128


def flip(index, bit):
    return index + bit - 2 * bit * ((index // bit) % 2)


def layer_kernel(
    dims,
    residual_hbm,
    pool_hbm,
    docs_hbm,
    map_hbm,
    scale_hbm,
    weight_hbm,
    mix_gain_hbm,
    mix_shift_hbm,
    group_router_hbm,
    expert_router_hbm,
    routes_hbm,
    own_gate,
    own_up,
    own_down,
    gain_hbm,
    shift_hbm,
    out,
    residual,
    source,
    docs,
    pool_map,
    pool_scale,
    out_weight,
    mix_gain,
    mix_shift,
    group_router,
    expert_router,
    routes,
    gain,
    shift,
    mixed_out,
    mixed_in,
    values,
    normed,
    meta,
    gate_a,
    up_a,
    down_a,
    gate_b,
    up_b,
    down_b,
    rows_in,
    meta_in,
    picked,
    spread,
    slot_weight,
    hidden,
    weighted,
    partial,
    passing,
    arrived,
    load_sems,
    send_sems,
    recv_sems,
):
    slots, expert_count = dims
    rows, width = normed.shape
    half = rows // 2
    ff = own_gate.shape[2]
    seq_rows, group_width = pool_hbm.shape
    reach = 16
    sp, tp = lax.axis_index("sp"), lax.axis_index("tp")
    sp_count = expert_count
    to_y = {"sp": flip(sp, 1)}
    to_z = {"sp": flip(sp, 2)}
    to_far = {"sp": flip(sp, group_size)}
    to_next = {"sp": (sp + 1) % sp_count}
    to_last = {"sp": (sp + sp_count - 1) % sp_count}
    to_x = {"tp": flip(tp, 2)}
    to_core = {"tp": flip(tp, 1)}
    to_diag = {"tp": flip(flip(tp, 2), 1)}
    inner = ((sp // 2 + 1) // 2) % 2 == 1

    barrier = pltpu.get_barrier_semaphore()
    peers = (to_y, to_z, to_far, to_next, to_last, to_x, to_core, to_diag)
    for peer in peers:
        pl.semaphore_signal(barrier, inc=1, device_id=peer, device_id_type=MESH)

    loads = []

    def load(src, dst):
        copy = pltpu.make_async_copy(src, dst, load_sems.at[len(loads)])
        copy.start()
        loads.append(copy)
        return copy

    load_source = load(pool_hbm, source.at[pl.ds(block, seq_rows)])
    load_docs = load(docs_hbm, docs.at[pl.ds(8, 8)])
    load_map = load(map_hbm.at[0], pool_map)
    load_scale = load(scale_hbm, pool_scale)
    front = [
        load(residual_hbm, residual),
        load(weight_hbm, out_weight),
        load(mix_gain_hbm, mix_gain),
        load(mix_shift_hbm, mix_shift),
        load(group_router_hbm, group_router),
        load(expert_router_hbm, expert_router),
        load(routes_hbm, routes),
    ]
    experts_in = [
        load(own_gate.at[0], gate_a),
        load(own_up.at[0], up_a),
        load(own_down.at[0], down_a),
    ]
    ends = [load(gain_hbm, gain), load(shift_hbm, shift)]

    source[pl.ds(0, block - reach), :] = jnp.zeros((block - reach, group_width), jnp.bfloat16)
    pl.semaphore_wait(barrier, len(peers))

    made = []

    def send(src, dst, peer, when=None):
        index = len(made)
        copy = pltpu.make_async_remote_copy(
            src_ref=src,
            dst_ref=dst,
            send_sem=send_sems.at[index],
            recv_sem=recv_sems.at[index],
            device_id=peer,
            device_id_type=MESH,
        )
        made.append(copy)
        if when is None:
            copy.start()
        else:
            pl.when(when)(copy.start)
        return copy

    tail_rows = send(
        pool_hbm.at[pl.ds(seq_rows - reach, reach)], source.at[pl.ds(block - reach, reach)], to_next
    )
    tail_docs = send(docs_hbm, docs.at[pl.ds(0, 8)], to_next)

    piece = ff // 4
    k_half = width // 2

    def cols(position):
        return pl.ds(pl.multiple_of(position * piece, piece), piece)

    mine, across = cols(tp), cols(flip(tp, 2))
    chunks = []
    for own, kept in ((own_gate, gate_b), (own_up, up_b)):
        for part in range(2):
            where = pl.ds(part * k_half, k_half)
            chunks.append(
                (own.at[0, where, mine], kept.at[where, mine], kept.at[where, across])
            )
    for part in range(2):
        where = pl.ds(part * k_half, k_half)
        chunks.append(
            (own_down.at[0, mine, where], down_b.at[mine, where], down_b.at[across, where])
        )
    far = [
        send(own, kept, to_far, None if index == 0 else inner)
        for index, (own, kept, beside) in enumerate(chunks)
    ]

    window = 2 * (1 + tp % 2) * (1 + 3 * (tp // 2))
    row_ids = lax.broadcasted_iota(jnp.int32, (block, 2 * block), 0)
    col_ids = lax.broadcasted_iota(jnp.int32, (block, 2 * block), 1)
    behind = row_ids + block - col_ids
    in_window = (behind >= 0) & (behind < window)
    first, second = pl.ds(0, half), pl.ds(half, half)
    halves = (first, second)
    destinations = (
        (flip(tp, 2), to_x),
        (flip(flip(tp, 2), 1), to_diag),
        (flip(tp, 1), to_core),
        (tp, None),
    )
    channels = pl.ds(pl.multiple_of(tp * group_width, group_width), group_width)
    load_source.wait()
    load_docs.wait()
    load_map.wait()
    load_scale.wait()

    mixed_sent = {0: [], 1: []}

    def mix(which):
        for owner, peer in destinations:
            index = owner * 2 + which
            start = pl.multiple_of(index * block, block)
            here = docs[pl.ds(index + 8, 1), :].astype(jnp.float32)
            before = docs[pl.ds(index + 7, 1), :].astype(jnp.float32)
            across_docs = jnp.concatenate([before, here], axis=1)
            down_docs = jnp.transpose(jnp.broadcast_to(here, (block, block)))
            down_docs = jnp.concatenate([down_docs, down_docs], axis=1)
            known = col_ids + (sp * seq_rows + start) >= block
            keep = jnp.where(in_window & known & (across_docs == down_docs), 1.0, 0.0)
            total = jnp.dot(
                keep.astype(jnp.bfloat16),
                source[pl.ds(start, 2 * block), :],
                preferred_element_type=jnp.float32,
            )
            count = jnp.sum(keep, axis=1, keepdims=True)
            center = source[pl.ds(start + block, block), :].astype(jnp.float32)
            pooled = (total / count - center).astype(jnp.bfloat16)
            mixed = jnp.dot(pooled, pool_map[...], preferred_element_type=jnp.float32)
            mixed = (mixed * pool_scale[...]).astype(jnp.bfloat16)
            if peer is None:
                mixed_in[which, :, channels] = mixed
            else:
                place = len(mixed_sent[0]) + len(mixed_sent[1])
                mixed_out[place] = mixed
                mixed_sent[which].append(
                    send(mixed_out.at[place], mixed_in.at[which, :, channels], peer)
                )

    mix(1)
    tail_rows.wait_recv()
    tail_docs.wait_recv()
    mix(0)

    slot_cols = lax.broadcasted_iota(jnp.int32, (half, half), 1)
    slot_rows = lax.broadcasted_iota(jnp.int32, (half, half), 0)
    earlier = jnp.where(slot_rows < slot_cols, 1.0, 0.0).astype(jnp.bfloat16)
    expert_ids = lax.broadcasted_iota(jnp.int32, (expert_count, half), 0)
    group_count = group_router.shape[0]
    transposed = (((1,), (1,)), ((), ()))

    def project(which):
        where = halves[which]
        for copy in mixed_sent[which]:
            copy.wait_recv()

        @pl.loop(0, 4)
        def _(step):
            wide = width // 4
            part = pl.ds(pl.multiple_of(step * wide, wide), wide)
            values[:, part] = skip_scale * residual[where, part].astype(jnp.float32) + jnp.dot(
                mixed_in[which], out_weight[:, part], preferred_element_type=jnp.float32
            )

        @pl.loop(0, half // 32)
        def _(step):
            part = pl.ds(pl.multiple_of(step * 32, 32), 32)
            normed[pl.ds(pl.multiple_of(which * half + step * 32, 32), 32), :] = layer_norm(
                values[part, :], mix_gain[...], mix_shift[...]
            ).astype(jnp.bfloat16)

    def route(which):
        where = halves[which]
        lines = normed[where, :]
        group_logits = lax.dot_general(
            group_router[...], lines, transposed, preferred_element_type=jnp.float32
        )
        expert_logits = lax.dot_general(
            expert_router[...], lines, transposed, preferred_element_type=jnp.float32
        )
        group_exp = jnp.exp(group_logits)
        group_prob = group_exp / jnp.sum(group_exp, axis=0, keepdims=True)
        named = (routes[0:1, where] == expert_ids) | (routes[1:2, where] == expert_ids)
        group_share = jnp.zeros((expert_count, half), jnp.float32)
        for group in range(group_count):
            group_share = jnp.where(
                expert_ids // (expert_count // group_count) == group,
                group_prob[group : group + 1, :],
                group_share,
            )
        picked_exp = jnp.where(named, jnp.exp(jnp.where(named, expert_logits, 0.0)), 0.0)
        share = group_share * (picked_exp / jnp.sum(picked_exp, axis=0, keepdims=True))
        ones = jnp.where(named, 1.0, 0.0)
        rank = jnp.dot(ones.astype(jnp.bfloat16), earlier, preferred_element_type=jnp.float32)
        meta[which, pl.ds(0, expert_count), :] = jnp.where(named, rank, -1.0)
        meta[which, pl.ds(expert_count, expert_count), :] = share

    for copy in front:
        copy.wait()
    rows_y, rows_z, meta_y, meta_z = {}, {}, {}, {}
    for which in (1, 0):
        where = halves[which]
        project(which)
        rows_y[which] = send(normed.at[where], rows_in.at[0, where], to_y)
        rows_z[which] = send(normed.at[where], rows_in.at[1, where], to_z)
        route(which)
        meta_y[which] = send(meta.at[which], meta_in.at[0, which], to_y)
        meta_z[which] = send(meta.at[which], meta_in.at[1, which], to_z)

    slot_ids = lax.broadcasted_iota(jnp.int32, (slots, half), 0).astype(jnp.float32)
    experts = (sp, flip(sp, group_size))

    def select(position, which, row_ref, meta_ref):
        parts = []
        for kind in range(2):
            slot_row = meta_ref[which, pl.ds(experts[kind], 1), :]
            weight_row = meta_ref[which, pl.ds(expert_count + experts[kind], 1), :]
            match = jnp.where(slot_ids == slot_row, 1.0, 0.0)
            slot_weight[kind, position, pl.ds(which * slots, slots), :] = jnp.sum(
                match * weight_row, axis=1, keepdims=True
            )
            parts.append(match)
        match = jnp.concatenate(parts, axis=0)
        spread[position, which] = jnp.transpose(match).astype(jnp.bfloat16)
        match = match.astype(jnp.bfloat16)

        @pl.loop(0, 4)
        def _(step):
            wide = width // 4
            part = pl.ds(pl.multiple_of(step * wide, wide), wide)
            found = jnp.dot(
                match, row_ref[halves[which], part], preferred_element_type=jnp.float32
            ).astype(jnp.bfloat16)
            for kind in range(2):
                picked[kind, position, pl.ds(which * slots, slots), part] = found[
                    kind * slots : (kind + 1) * slots
                ]

    def ffn(position, kind, gate, up, down):
        @pl.loop(0, 2)
        def _(step):
            wide = ff // 2
            part = pl.ds(pl.multiple_of(step * wide, wide), wide)
            lines = picked[kind, position]
            gate_out = jnp.dot(lines, gate[:, part], preferred_element_type=jnp.float32)
            up_out = jnp.dot(lines, up[:, part], preferred_element_type=jnp.float32)
            hidden[:, part] = (gate_out / (1.0 + jnp.exp(-gate_out)) * up_out).astype(jnp.bfloat16)

        @pl.loop(0, 4)
        def _(step):
            wide = width // 4
            part = pl.ds(pl.multiple_of(step * wide, wide), wide)
            result = jnp.dot(hidden[...], down[:, part], preferred_element_type=jnp.float32)
            result = (result * slot_weight[kind, position]).astype(jnp.bfloat16)
            for which in range(2):
                weighted[position, which, pl.ds(kind * slots, slots), part] = result[
                    which * slots : (which + 1) * slots
                ]

    def gather_back(position):
        for which in range(2):

            @pl.loop(0, 4)
            def _(step):
                wide = width // 4
                part = pl.ds(pl.multiple_of(step * wide, wide), wide)
                partial[position, halves[which], part] = jnp.dot(
                    spread[position, which],
                    weighted[position, which, :, part],
                    preferred_element_type=jnp.float32,
                ).astype(jnp.bfloat16)

    by_x, by_core, by_relay = [], [], []

    def pass_far(index):
        own, kept, beside = chunks[index]
        far[index].wait_recv()
        by_x.append(send(kept, kept, to_x))
        by_core.append(send(kept, kept, to_core))

    def pass_x(index):
        own, kept, beside = chunks[index]
        by_x[index].wait_recv()
        by_relay.append(send(beside, beside, to_core))

    own, from_y, from_z, from_corner = 3, 0, 1, 2
    select(own, 1, normed, meta)
    select(own, 0, normed, meta)
    for copy in experts_in:
        copy.wait()
    ffn(own, 0, gate_a, up_a, down_a)
    pass_far(0)

    rows_y[1].wait_recv()
    meta_y[1].wait_recv()
    corner_1 = send(rows_in.at[0, second], rows_in.at[2, second], to_z)
    corner_meta_1 = send(meta_in.at[0, 1], meta_in.at[2, 1], to_z)
    for index in range(1, len(chunks)):
        pl.when(jnp.logical_not(inner))(far[index].start)
    select(from_y, 1, rows_in.at[0], meta_in.at[0])
    rows_z[1].wait_recv()
    meta_z[1].wait_recv()
    select(from_z, 1, rows_in.at[1], meta_in.at[1])
    pass_x(0)
    rows_z[0].wait_recv()
    meta_z[0].wait_recv()
    corner_0 = send(rows_in.at[1, first], rows_in.at[2, first], to_y)
    corner_meta_0 = send(meta_in.at[1, 0], meta_in.at[2, 0], to_y)
    select(from_z, 0, rows_in.at[1], meta_in.at[1])
    ffn(from_z, 0, gate_a, up_a, down_a)
    rows_y[0].wait_recv()
    meta_y[0].wait_recv()
    select(from_y, 0, rows_in.at[0], meta_in.at[0])
    ffn(from_y, 0, gate_a, up_a, down_a)
    corner_1.wait_recv()
    corner_meta_1.wait_recv()
    select(from_corner, 1, rows_in.at[2], meta_in.at[2])
    corner_0.wait_recv()
    corner_meta_0.wait_recv()
    select(from_corner, 0, rows_in.at[2], meta_in.at[2])
    ffn(from_corner, 0, gate_a, up_a, down_a)
    for index in range(1, len(chunks)):
        pass_far(index)
        if index > 1:
            pass_x(index - 1)
    pass_x(len(chunks) - 1)
    for copy in by_core + by_relay:
        copy.wait_recv()

    ffn(from_corner, 1, gate_b, up_b, down_b)
    gather_back(from_corner)
    pass_y = send(partial.at[from_corner, first], passing.at[0], to_y)
    pass_z = send(partial.at[from_corner, second], passing.at[1], to_z)
    ffn(from_y, 1, gate_b, up_b, down_b)
    gather_back(from_y)
    back_y1 = send(partial.at[from_y, first], arrived.at[0, first], to_y)
    ffn(from_z, 1, gate_b, up_b, down_b)
    gather_back(from_z)
    back_z2 = send(partial.at[from_z, second], arrived.at[1, second], to_z)

    def add_passing(position, where, slot):
        partial[position, where, :] = (
            partial[position, where, :].astype(jnp.float32) + passing[slot].astype(jnp.float32)
        ).astype(jnp.bfloat16)

    ffn(own, 1, gate_b, up_b, down_b)
    pass_y.wait_recv()
    add_passing(from_z, first, 0)
    back_z1 = send(partial.at[from_z, first], arrived.at[1, first], to_z)
    pass_z.wait_recv()
    add_passing(from_y, second, 1)
    back_y2 = send(partial.at[from_y, second], arrived.at[0, second], to_y)
    for copy in ends:
        copy.wait()
    for copy in (back_y1, back_z2, back_z1, back_y2):
        copy.wait_recv()

    for which in range(2):

        @pl.loop(0, half // 64)
        def _(step):
            inside = pl.ds(pl.multiple_of(step * 64, 64), 64)
            part = pl.ds(pl.multiple_of(which * half + step * 64, 64), 64)
            routed = jnp.dot(
                spread[own, which, inside, :],
                weighted[own, which],
                preferred_element_type=jnp.float32,
            )
            routed = routed + arrived[0, part, :].astype(jnp.float32)
            routed = routed + arrived[1, part, :].astype(jnp.float32)
            total = skip_scale * normed[part, :].astype(jnp.float32) + routed
            out[part, :] = layer_norm(total, gain[...], shift[...]).astype(jnp.bfloat16)

    for copy in made:
        copy.wait_send()


def near_layer(
    residual,
    pool_input,
    doc_ids,
    pool_map,
    pool_scale,
    out_weight,
    mix_gain,
    mix_shift,
    group_router,
    expert_router,
    expert_gate,
    expert_up,
    expert_down,
    routes,
    ffn_gain,
    ffn_shift,
):
    expert_count = lax.axis_size("sp")
    rows, width = residual.shape
    ff = expert_gate.shape[2]
    seq_rows, group_width = pool_input.shape
    pool_width = out_weight.shape[0]
    group_count = group_router.shape[1]
    half = rows // 2
    slots = half * routes.shape[1] * 2 // expert_count
    anywhere = pl.BlockSpec(memory_space=pl.ANY)
    bf16, f32 = jnp.bfloat16, jnp.float32
    operands = (
        residual,
        pool_input,
        doc_ids.reshape(seq_rows // block, block),
        pool_map,
        pool_scale[None, :],
        out_weight,
        mix_gain[None, :],
        mix_shift[None, :],
        group_router.T,
        expert_router.T,
        routes.T,
        expert_gate,
        expert_up,
        expert_down,
        ffn_gain[None, :],
        ffn_shift[None, :],
    )
    return pl.pallas_call(
        functools.partial(layer_kernel, (slots, expert_count)),
        out_shape=jax.ShapeDtypeStruct((rows, width), bf16),
        in_specs=[anywhere] * len(operands),
        out_specs=pl.BlockSpec(memory_space=pltpu.VMEM),
        scratch_shapes=[
            pltpu.VMEM((rows, width), bf16),
            pltpu.VMEM((seq_rows + block, group_width), bf16),
            pltpu.VMEM((16, block), jnp.int32),
            pltpu.VMEM((group_width, group_width), bf16),
            pltpu.VMEM((1, group_width), f32),
            pltpu.VMEM((pool_width, width), bf16),
            pltpu.VMEM((1, width), f32),
            pltpu.VMEM((1, width), f32),
            pltpu.VMEM((group_count, width), bf16),
            pltpu.VMEM((expert_count, width), bf16),
            pltpu.VMEM(routes.shape[::-1], jnp.int32),
            pltpu.VMEM((1, width), f32),
            pltpu.VMEM((1, width), f32),
            pltpu.VMEM((6, block, group_width), bf16),
            pltpu.VMEM((2, half, pool_width), bf16),
            pltpu.VMEM((half, width), f32),
            pltpu.VMEM((rows, width), bf16),
            pltpu.VMEM((2, 2 * expert_count, half), f32),
            pltpu.VMEM((width, ff), bf16),
            pltpu.VMEM((width, ff), bf16),
            pltpu.VMEM((ff, width), bf16),
            pltpu.VMEM((width, ff), bf16),
            pltpu.VMEM((width, ff), bf16),
            pltpu.VMEM((ff, width), bf16),
            pltpu.VMEM((3, rows, width), bf16),
            pltpu.VMEM((3, 2, 2 * expert_count, half), f32),
            pltpu.VMEM((2, 4, 2 * slots, width), bf16),
            pltpu.VMEM((4, 2, half, 2 * slots), bf16),
            pltpu.VMEM((2, 4, 2 * slots, 1), f32),
            pltpu.VMEM((2 * slots, ff), bf16),
            pltpu.VMEM((4, 2, 2 * slots, width), bf16),
            pltpu.VMEM((3, rows, width), bf16),
            pltpu.VMEM((2, half, width), bf16),
            pltpu.VMEM((2, rows, width), bf16),
            pltpu.SemaphoreType.DMA((16,)),
            pltpu.SemaphoreType.DMA((64,)),
            pltpu.SemaphoreType.DMA((64,)),
        ],
        compiler_params=pltpu.CompilerParams(
            collective_id=0, has_side_effects=True, vmem_limit_bytes=60 * 1024 * 1024
        ),
    )(*operands)


def on_device(
    residual,
    pool_input,
    doc_ids,
    pool_map,
    pool_scale,
    out_weight,
    mix_gain,
    mix_shift,
    group_router,
    expert_router,
    expert_gate,
    expert_up,
    expert_down,
    routes,
    ffn_gain,
    ffn_shift,
):
    seq_rows = pool_input.shape[0]
    reach_rows = 15
    expert_count = lax.axis_size("sp")
    tp_count = lax.axis_size("tp")
    near = expert_count == 2 * group_size and tp_count == group_size
    near = near and residual.shape[0] == 2 * block and seq_rows == tp_count * residual.shape[0]
    if near:
        return near_layer(
            residual,
            pool_input,
            doc_ids,
            pool_map,
            pool_scale,
            out_weight,
            mix_gain,
            mix_shift,
            group_router,
            expert_router,
            expert_gate,
            expert_up,
            expert_down,
            routes,
            ffn_gain,
            ffn_shift,
        )
    window = jnp.left_shift(jnp.int32(2), lax.axis_index("tp"))
    first_row = lax.axis_index("sp") * seq_rows
    tail_values, tail_docs = from_behind(
        (pool_input[seq_rows - reach_rows :], doc_ids[seq_rows - reach_rows :]), "sp", 1
    )
    source = jnp.concatenate([tail_values, pool_input], axis=0).astype(jnp.float32)
    all_docs = jnp.concatenate([tail_docs, doc_ids], axis=0)
    positions = first_row - reach_rows + jnp.arange(seq_rows + reach_rows, dtype=jnp.int32)
    running = jnp.zeros((seq_rows, source.shape[1]), jnp.float32)
    weight_sum = jnp.zeros((seq_rows, 1), jnp.float32)
    for offset in range(reach_rows + 1):
        begin_row = reach_rows - offset
        earlier = source[begin_row : begin_row + seq_rows]
        keep_mask = (
            (all_docs[begin_row : begin_row + seq_rows] == doc_ids)
            & (positions[begin_row : begin_row + seq_rows] >= 0)
            & (offset < window)
        )
        same_doc = keep_mask.astype(jnp.float32)[:, None]
        running = running + same_doc * earlier
        weight_sum = weight_sum + same_doc
    pooled = (running / weight_sum - source[reach_rows:]).astype(jnp.bfloat16)
    mixed = (jnp.dot(pooled, pool_map[0], preferred_element_type=jnp.float32) * pool_scale).astype(
        jnp.bfloat16
    )
    row_count = seq_rows // tp_count
    blocks = mixed.reshape(tp_count, row_count, mixed.shape[1])
    branch = jnp.einsum(
        "abc,cd->abd",
        lax.all_to_all(blocks, "tp", split_axis=0, concat_axis=2, tiled=True),
        out_weight,
        preferred_element_type=jnp.float32,
    )[0]
    normed = layer_norm(
        skip_scale * residual.astype(jnp.float32) + branch, mix_gain, mix_shift
    ).astype(jnp.bfloat16)
    weight = route_weights(normed, routes, group_router, expert_router)
    half_most = row_count * routes.shape[1] // expert_count
    half_rows = row_count // 2
    routed_parts = []
    for piece_index in range(2):
        rows_here = slice(piece_index * half_rows, (piece_index + 1) * half_rows)
        outgoing, slot_index = fill_slots(
            normed[rows_here], routes[rows_here], half_most, expert_count
        )
        returned = lax.all_to_all(
            expert_ffn(
                lax.all_to_all(outgoing, "sp", split_axis=0, concat_axis=0, tiled=True),
                expert_gate,
                expert_up,
                expert_down,
            ),
            "sp",
            split_axis=0,
            concat_axis=0,
            tiled=True,
        )
        routed_parts.append(combine_rows(returned, slot_index, weight[rows_here]))
    routed = jnp.concatenate(routed_parts, axis=0)
    return layer_norm(skip_scale * normed.astype(jnp.float32) + routed, ffn_gain, ffn_shift).astype(
        jnp.bfloat16
    )


def solution(mesh):
    in_specs = (
        P(("sp", "tp"), None),
        P("sp", "tp"),
        P("sp"),
        P("tp", None, None),
        P("tp"),
        P(),
        P(),
        P(),
        P(),
        P(),
        P("sp", None, None),
        P("sp", None, None),
        P("sp", None, None),
        P(("sp", "tp"), None),
        P(),
        P(),
    )
    out_specs = P(("sp", "tp"), None)
    return jax.shard_map(
        on_device, mesh=mesh, in_specs=in_specs, out_specs=out_specs, check_vma=False
    )
```

```python
import functools

import jax
import jax.numpy as jnp
from jax import lax
from jax.experimental import pallas as pl
from jax.experimental.pallas import tpu as pltpu
from jax.sharding import PartitionSpec as P

skip_scale = 2.0**0.5
epsilon = 1e-05


def from_behind(block, axis, distance):
    devices = range(lax.axis_size(axis))
    route = [(i - distance, i) for i in devices if i - distance in devices]
    return lax.ppermute(block, axis, route)


def layer_norm(values, norm_gain, norm_shift):
    center = values - jnp.mean(values, axis=-1, keepdims=True)
    spread = jnp.mean(center * center, axis=-1, keepdims=True)
    return center * lax.rsqrt(spread + epsilon) * norm_gain + norm_shift


def route_weights(normed, chosen, group_router, expert_router):
    group_logits = jnp.dot(normed, group_router, preferred_element_type=jnp.float32)
    expert_logits = jnp.dot(normed, expert_router, preferred_element_type=jnp.float32)
    group_count = group_logits.shape[1]
    expert_count = expert_logits.shape[1]
    group_exp = jnp.exp(group_logits)
    group_prob = group_exp / jnp.sum(group_exp, axis=1, keepdims=True)
    expert_ids = jnp.arange(expert_count, dtype=jnp.int32)
    picked = jnp.sum(
        jnp.where(chosen[:, :, None] == expert_ids[None, None, :], expert_logits[:, None, :], 0.0),
        axis=2,
    )
    picked_exp = jnp.exp(picked)
    pair_share = picked_exp / jnp.sum(picked_exp, axis=1, keepdims=True)
    group_of = chosen // (expert_count // group_count)
    group_ids = jnp.arange(group_count, dtype=jnp.int32)
    group_share = jnp.sum(
        jnp.where(group_of[:, :, None] == group_ids[None, None, :], group_prob[:, None, :], 0.0),
        axis=2,
    )
    return group_share * pair_share


def expert_ffn(arrived, expert_gate, expert_up, expert_down):
    sources, slot_count, width = arrived.shape
    gathered = arrived.reshape(sources * slot_count, width)
    gate_out = jnp.dot(gathered, expert_gate[0], preferred_element_type=jnp.float32)
    up_out = jnp.dot(gathered, expert_up[0], preferred_element_type=jnp.float32)
    hidden = (jax.nn.silu(gate_out) * up_out).astype(jnp.bfloat16)
    result = jnp.dot(hidden, expert_down[0], preferred_element_type=jnp.float32).astype(
        jnp.bfloat16
    )
    return result.reshape(sources, slot_count, width)


def fill_slots(normed, chosen, capacity, expert_count):
    flat_routes = chosen.reshape(-1)
    entry_count = flat_routes.shape[0]
    onehot = (flat_routes[:, None] == jnp.arange(expert_count, dtype=jnp.int32)[None, :]).astype(
        jnp.int32
    )
    slot_rank = jnp.sum((jnp.cumsum(onehot, axis=0) - onehot) * onehot, axis=1)
    slot_index = flat_routes * capacity + slot_rank
    token_ids = jnp.arange(entry_count, dtype=jnp.int32) // chosen.shape[1]
    source_row = (
        jnp.full((expert_count * capacity,), normed.shape[0], jnp.int32)
        .at[slot_index]
        .set(token_ids)
    )
    padded = jnp.concatenate([normed, jnp.zeros((1, normed.shape[1]), normed.dtype)], axis=0)
    outgoing = jnp.take(padded, source_row, axis=0).reshape(expert_count, capacity, normed.shape[1])
    return (outgoing, slot_index)


def combine_rows(returned, slot_index, weight):
    flat_out = returned.reshape(-1, returned.shape[2])
    picked = jnp.take(flat_out, slot_index, axis=0).reshape(
        weight.shape[0], weight.shape[1], flat_out.shape[1]
    )
    return jnp.sum(weight[:, :, None] * picked.astype(jnp.float32), axis=1)


MESH = pl.DeviceIdType.MESH
group_size = 4
block = 128


def flip(index, bit):
    return index + bit - 2 * bit * ((index // bit) % 2)


def opposite(index):
    return flip(flip(index, 2), group_size)


def layer_kernel(
    dims,
    residual_hbm,
    pool_hbm,
    docs_hbm,
    map_hbm,
    scale_hbm,
    weight_hbm,
    mix_gain_hbm,
    mix_shift_hbm,
    group_router_hbm,
    expert_router_hbm,
    routes_hbm,
    own_gate,
    own_up,
    own_down,
    gain_hbm,
    shift_hbm,
    out,
    residual,
    source,
    docs,
    pool_map,
    pool_scale,
    out_weight,
    mix_gain,
    mix_shift,
    group_router,
    expert_router,
    routes,
    gain,
    shift,
    mixed_out,
    mixed_in,
    values,
    normed,
    meta,
    gate_a,
    up_a,
    down_a,
    gate_b,
    up_b,
    down_b,
    rows_in,
    meta_in,
    picked,
    spread,
    slot_weight,
    hidden,
    weighted,
    partial,
    passing,
    arrived,
    hidden_out,
    hidden_in,
    late_a,
    late_b,
    late_spread,
    late_weight,
    late_rows,
    load_sems,
    send_sems,
    recv_sems,
):
    slots, expert_count = dims
    rows, width = normed.shape
    half = rows // 2
    ff = own_gate.shape[2]
    seq_rows, group_width = pool_hbm.shape
    reach = 16
    back_y = rows // 2
    sp, tp = lax.axis_index("sp"), lax.axis_index("tp")
    sp_count = expert_count
    to_y = {"sp": flip(sp, 1)}
    to_z = {"sp": flip(sp, 2)}
    to_far = {"sp": opposite(sp)}
    to_next = {"sp": (sp + 1) % sp_count}
    to_last = {"sp": (sp + sp_count - 1) % sp_count}
    to_x = {"tp": flip(tp, 2)}
    to_core = {"tp": flip(tp, 1)}
    to_corner = {"sp": flip(flip(sp, 1), 2)}
    to_diag = {"tp": flip(flip(tp, 2), 1)}
    inner = ((sp // 2 + 1) // 2) % 2 == 1

    barrier = pltpu.get_barrier_semaphore()
    peers = (to_y, to_z, to_corner, to_far, to_next, to_last, to_x, to_core, to_diag)
    for peer in peers:
        pl.semaphore_signal(barrier, inc=1, device_id=peer, device_id_type=MESH)

    loads = []

    def load(src, dst):
        copy = pltpu.make_async_copy(src, dst, load_sems.at[len(loads)])
        copy.start()
        loads.append(copy)
        return copy

    load_source = load(pool_hbm, source.at[pl.ds(block, seq_rows)])
    load_docs = load(docs_hbm, docs.at[pl.ds(8, 8)])
    load_map = load(map_hbm.at[0], pool_map)
    load_scale = load(scale_hbm, pool_scale)
    front = [
        load(residual_hbm, residual),
        load(weight_hbm, out_weight),
        load(mix_gain_hbm, mix_gain),
        load(mix_shift_hbm, mix_shift),
        load(group_router_hbm, group_router),
        load(expert_router_hbm, expert_router),
        load(routes_hbm, routes),
    ]
    experts_in = [
        load(own_gate.at[0], gate_a),
        load(own_up.at[0], up_a),
        load(own_down.at[0], down_a),
    ]
    ends = [load(gain_hbm, gain), load(shift_hbm, shift)]

    source[pl.ds(0, block - reach), :] = jnp.zeros((block - reach, group_width), jnp.bfloat16)
    pl.semaphore_wait(barrier, len(peers))

    made = []

    def send(src, dst, peer, when=None, start=True):
        index = len(made)
        copy = pltpu.make_async_remote_copy(
            src_ref=src,
            dst_ref=dst,
            send_sem=send_sems.at[index],
            recv_sem=recv_sems.at[index],
            device_id=peer,
            device_id_type=MESH,
        )
        made.append((copy, when))
        if start and when is None:
            copy.start()
        elif start:
            pl.when(when)(copy.start)
        return copy

    tail_rows = send(
        pool_hbm.at[pl.ds(seq_rows - reach, reach)], source.at[pl.ds(block - reach, reach)], to_next
    )
    tail_docs = send(docs_hbm, docs.at[pl.ds(0, 8)], to_next)

    quarter = width // 4
    late = ff // 2

    def share(position):
        return pl.ds(pl.multiple_of(position * quarter, quarter), quarter)

    mine, across = share(tp), share(flip(tp, 2))
    soon, later = pl.ds(0, late), pl.ds(late, late)
    outer = jnp.logical_not(inner)
    chunks = [
        (own_gate.at[0, mine, soon], gate_b.at[mine, soon], gate_b.at[across, soon], None),
        (own_up.at[0, mine, soon], up_b.at[mine, soon], up_b.at[across, soon], None),
        (own_down.at[0, soon, mine], down_b.at[soon, mine], down_b.at[soon, across], None),
        (own_gate.at[0, mine, later], gate_b.at[mine, later], gate_b.at[across, later], None),
        (own_up.at[0, mine, later], up_b.at[mine, later], up_b.at[across, later], None),
        (own_down.at[0, later, mine], down_b.at[later, mine], down_b.at[later, across], inner),
        (own_down.at[0, later, mine], late_a.at[:, mine], late_a.at[:, across], outer),
    ]
    far = [
        send(own_part, kept, to_far, when, start=False)
        for own_part, kept, beside, when in chunks
    ]
    by_x = [
        send(kept, kept, to_x, inner if when is inner else None, start=False)
        for own_part, kept, beside, when in chunks
    ]
    by_core = [
        send(kept, kept, to_core, inner if when is inner else None, start=False)
        for own_part, kept, beside, when in chunks
    ]
    by_relay = [
        send(beside, beside, to_core, inner if when is inner else None, start=False)
        for own_part, kept, beside, when in chunks
    ]

    def start_far(indices, when):
        @pl.when(when)
        def _():
            for index in indices:
                far[index].start()

    start_far((0, 1, 2), outer)
    start_far((0, 1, 2, 3, 4, 5), inner)

    window = 2 * (1 + tp % 2) * (1 + 3 * (tp // 2))
    row_ids = lax.broadcasted_iota(jnp.int32, (block, 2 * block), 0)
    col_ids = lax.broadcasted_iota(jnp.int32, (block, 2 * block), 1)
    behind = row_ids + block - col_ids
    in_window = (behind >= 0) & (behind < window)
    first, second = pl.ds(0, half), pl.ds(half, half)
    halves = (first, second)
    destinations = (
        (flip(tp, 2), to_x),
        (flip(flip(tp, 2), 1), to_diag),
        (flip(tp, 1), to_core),
        (tp, None),
    )
    channels = pl.ds(pl.multiple_of(tp * group_width, group_width), group_width)
    load_source.wait()
    load_docs.wait()
    load_map.wait()
    load_scale.wait()

    mixed_sent = {0: [], 1: []}

    def mix(which):
        for owner, peer in destinations:
            index = owner * 2 + which
            start = pl.multiple_of(index * block, block)
            here = docs[pl.ds(index + 8, 1), :].astype(jnp.float32)
            before = docs[pl.ds(index + 7, 1), :].astype(jnp.float32)
            across_docs = jnp.concatenate([before, here], axis=1)
            down_docs = jnp.transpose(jnp.broadcast_to(here, (block, block)))
            down_docs = jnp.concatenate([down_docs, down_docs], axis=1)
            known = col_ids + (sp * seq_rows + start) >= block
            keep = jnp.where(in_window & known & (across_docs == down_docs), 1.0, 0.0)
            total = jnp.dot(
                keep.astype(jnp.bfloat16),
                source[pl.ds(start, 2 * block), :],
                preferred_element_type=jnp.float32,
            )
            count = jnp.sum(keep, axis=1, keepdims=True)
            center = source[pl.ds(start + block, block), :].astype(jnp.float32)
            pooled = (total / count - center).astype(jnp.bfloat16)
            mixed = jnp.dot(pooled, pool_map[...], preferred_element_type=jnp.float32)
            mixed = (mixed * pool_scale[...]).astype(jnp.bfloat16)
            if peer is None:
                mixed_in[which, :, channels] = mixed
            else:
                place = len(mixed_sent[0]) + len(mixed_sent[1])
                mixed_out[place] = mixed
                mixed_sent[which].append(
                    send(mixed_out.at[place], mixed_in.at[which, :, channels], peer)
                )

    mix(1)
    tail_rows.wait_recv()
    tail_docs.wait_recv()
    mix(0)

    slot_cols = lax.broadcasted_iota(jnp.int32, (half, half), 1)
    slot_rows = lax.broadcasted_iota(jnp.int32, (half, half), 0)
    earlier = jnp.where(slot_rows < slot_cols, 1.0, 0.0).astype(jnp.bfloat16)
    expert_ids = lax.broadcasted_iota(jnp.int32, (expert_count, half), 0)
    group_count = group_router.shape[0]
    transposed = (((1,), (1,)), ((), ()))

    def project(which):
        where = halves[which]
        for copy in mixed_sent[which]:
            copy.wait_recv()

        @pl.loop(0, 4, unroll=2)
        def _(step):
            wide = width // 4
            part = pl.ds(pl.multiple_of(step * wide, wide), wide)
            values[where, part] = skip_scale * residual[where, part].astype(jnp.float32) + jnp.dot(
                mixed_in[which], out_weight[:, part], preferred_element_type=jnp.float32
            )

        @pl.loop(0, half // 16, unroll=2)
        def _(step):
            part = pl.ds(pl.multiple_of(which * half + step * 16, 16), 16)
            normed[part, :] = layer_norm(values[part, :], mix_gain[...], mix_shift[...]).astype(
                jnp.bfloat16
            )

    def route(which):
        where = halves[which]
        lines = normed[where, :]
        group_logits = lax.dot_general(
            group_router[...], lines, transposed, preferred_element_type=jnp.float32
        )
        expert_logits = lax.dot_general(
            expert_router[...], lines, transposed, preferred_element_type=jnp.float32
        )
        group_exp = jnp.exp(group_logits)
        group_prob = group_exp / jnp.sum(group_exp, axis=0, keepdims=True)
        named = (routes[0:1, where] == expert_ids) | (routes[1:2, where] == expert_ids)
        group_share = jnp.zeros((expert_count, half), jnp.float32)
        for group in range(group_count):
            group_share = jnp.where(
                expert_ids // (expert_count // group_count) == group,
                group_prob[group : group + 1, :],
                group_share,
            )
        picked_exp = jnp.where(named, jnp.exp(jnp.where(named, expert_logits, 0.0)), 0.0)
        share = group_share * (picked_exp / jnp.sum(picked_exp, axis=0, keepdims=True))
        ones = jnp.where(named, 1.0, 0.0)
        rank = jnp.dot(ones.astype(jnp.bfloat16), earlier, preferred_element_type=jnp.float32)
        meta[which, pl.ds(0, expert_count), :] = jnp.where(named, rank, -1.0)
        meta[which, pl.ds(expert_count, expert_count), :] = share

    for copy in front:
        copy.wait()
    rows_y, rows_z, meta_y, meta_z = {}, {}, {}, {}
    for which in (1, 0):
        where = halves[which]
        project(which)
        route(which)
        meta_y[which] = send(meta.at[which], meta_in.at[0, which], to_y)
        meta_z[which] = send(meta.at[which], meta_in.at[1, which], to_z)
        rows_y[which] = send(normed.at[where], rows_in.at[0, where], to_y)
        rows_z[which] = send(normed.at[where], rows_in.at[1, where], to_z)

    start_far((6,), outer)

    slot_ids = lax.broadcasted_iota(jnp.int32, (slots, half), 0).astype(jnp.float32)
    experts = (sp, opposite(sp))

    def select(position, which, row_ref, meta_ref):
        parts = []
        for kind in range(2):
            slot_row = meta_ref[which, pl.ds(experts[kind], 1), :]
            weight_row = meta_ref[which, pl.ds(expert_count + experts[kind], 1), :]
            match = jnp.where(slot_ids == slot_row, 1.0, 0.0)
            slot_weight[kind, position, pl.ds(which * slots, slots), :] = jnp.sum(
                match * weight_row, axis=1, keepdims=True
            )
            parts.append(match)
        match = jnp.concatenate(parts, axis=0)
        spread[position, which] = jnp.transpose(match).astype(jnp.bfloat16)
        match = match.astype(jnp.bfloat16)

        @pl.loop(0, 4, unroll=2)
        def _(step):
            wide = width // 4
            part = pl.ds(pl.multiple_of(step * wide, wide), wide)
            found = jnp.dot(
                match, row_ref[halves[which], part], preferred_element_type=jnp.float32
            ).astype(jnp.bfloat16)
            for kind in range(2):
                picked[kind, position, pl.ds(which * slots, slots), part] = found[
                    kind * slots : (kind + 1) * slots
                ]

    def activate(lines, gate, up):
        gate_out = jnp.dot(lines, gate, preferred_element_type=jnp.float32)
        up_out = jnp.dot(lines, up, preferred_element_type=jnp.float32)
        return (gate_out / (1.0 + jnp.exp(-gate_out)) * up_out).astype(jnp.bfloat16)

    def ffn(position, kind, gate, up, down, parts):
        depth = parts * late

        @pl.loop(0, parts)
        def _(step):
            part = pl.ds(pl.multiple_of(step * late, late), late)
            hidden[:, part] = activate(picked[kind, position], gate[:, part], up[:, part])

        @pl.loop(0, 4, unroll=2)
        def _(step):
            wide = width // 4
            part = pl.ds(pl.multiple_of(step * wide, wide), wide)
            result = jnp.dot(
                hidden[:, :depth], down[:depth, part], preferred_element_type=jnp.float32
            )
            result = (result * slot_weight[kind, position]).astype(jnp.bfloat16)
            for which in range(2):
                weighted[position, which, pl.ds(kind * slots, slots), part] = result[
                    which * slots : (which + 1) * slots
                ]

    own, from_y, from_z, from_corner = 3, 0, 1, 2

    def gather_back(position):
        for which in range(2):

            @pl.loop(0, 4, unroll=2)
            def _(step):
                wide = width // 4
                part = pl.ds(pl.multiple_of(step * wide, wide), wide)
                partial[position, halves[which], part] = jnp.dot(
                    spread[position, which],
                    weighted[position, which, :, part],
                    preferred_element_type=jnp.float32,
                ).astype(jnp.bfloat16)

    def start_sum(which):
        where = halves[which]

        @pl.loop(0, 4, unroll=2)
        def _(step):
            wide = width // 4
            part = pl.ds(pl.multiple_of(step * wide, wide), wide)
            values[where, part] = skip_scale * normed[where, part].astype(jnp.float32) + jnp.dot(
                spread[own, which], weighted[own, which, :, part], preferred_element_type=jnp.float32
            )

    def pass_far(index):
        far[index].wait_recv()
        by_x[index].start()
        by_core[index].start()

    def pass_x(index):
        by_x[index].wait_recv()
        by_relay[index].start()

    def settle(indices):
        for index in indices:
            by_core[index].wait_recv()
            by_relay[index].wait_recv()

    outermost = jnp.where(inner, flip(sp, 2), sp)
    keepers = (outermost, flip(outermost, 1))
    for which in range(2):
        parts = []
        for place, keeper in enumerate(keepers):
            expert = opposite(keeper)
            match = jnp.where(slot_ids == meta[which, pl.ds(expert, 1), :], 1.0, 0.0)
            late_weight[place, pl.ds(which * slots, slots), :] = jnp.sum(
                match * meta[which, pl.ds(expert_count + expert, 1), :], axis=1, keepdims=True
            )
            parts.append(match)
        late_spread[which] = jnp.transpose(jnp.concatenate(parts, axis=0)).astype(jnp.bfloat16)

    select(own, 1, normed, meta)
    select(own, 0, normed, meta)
    for copy in experts_in:
        copy.wait()
    ffn(own, 0, gate_a, up_a, down_a, 2)

    y_part, z_part = pl.ds(0, back_y), pl.ds(back_y, rows - back_y)
    corner_meta_1 = send(meta_in.at[0, 1], meta_in.at[2, 1], to_z, start=False)
    corner_meta_0 = send(meta_in.at[1, 0], meta_in.at[2, 0], to_y, start=False)
    corner_1 = send(rows_in.at[1, second], rows_in.at[2, second], to_y, start=False)
    corner_0 = send(rows_in.at[1, first], rows_in.at[2, first], to_y, start=False)
    late_z = send(late_a.at[:, mine], late_a.at[:, mine], to_z, outer, start=False)
    late_y = send(late_a.at[:, mine], late_b.at[:, mine], to_y, start=False)
    late_x = send(late_b.at[:, mine], late_b.at[:, mine], to_x, start=False)
    late_core = send(late_b.at[:, mine], late_b.at[:, mine], to_core, start=False)
    late_relay = send(late_b.at[:, across], late_b.at[:, across], to_core, start=False)
    pass_y = send(partial.at[from_corner, y_part], passing.at[y_part], to_y, start=False)
    pass_z = send(partial.at[from_corner, z_part], passing.at[z_part], to_z, start=False)
    back_y1 = send(partial.at[from_y, y_part], arrived.at[0, y_part], to_y, start=False)
    back_z1 = send(partial.at[from_z, z_part], arrived.at[1, z_part], to_z, start=False)
    back_y2 = send(partial.at[from_y, z_part], arrived.at[0, z_part], to_y, start=False)
    back_z2 = send(partial.at[from_z, y_part], arrived.at[1, y_part], to_z, start=False)
    hidden_y = send(hidden_out.at[0], hidden_in.at[1], to_y, outer, start=False)
    hidden_z = send(hidden_out.at[1], hidden_in.at[0], to_z, outer, start=False)
    hidden_corner = send(hidden_out.at[2], hidden_in.at[1], to_corner, outer, start=False)

    def take_y1():
        meta_y[1].wait_recv()
        corner_meta_1.start()
        rows_y[1].wait_recv()
        select(from_y, 1, rows_in.at[0], meta_in.at[0])

    def take_y0():
        meta_y[0].wait_recv()
        rows_y[0].wait_recv()
        select(from_y, 0, rows_in.at[0], meta_in.at[0])
        ffn(from_y, 0, gate_a, up_a, down_a, 2)

    def take_z1():
        meta_z[1].wait_recv()
        rows_z[1].wait_recv()
        corner_1.start()
        select(from_z, 1, rows_in.at[1], meta_in.at[1])

    def take_z0():
        meta_z[0].wait_recv()
        corner_meta_0.start()
        rows_z[0].wait_recv()
        corner_0.start()
        select(from_z, 0, rows_in.at[1], meta_in.at[1])
        ffn(from_z, 0, gate_a, up_a, down_a, 2)

    def take_corner1():
        corner_meta_1.wait_recv()
        corner_1.wait_recv()
        select(from_corner, 1, rows_in.at[2], meta_in.at[2])

    def take_corner0():
        corner_meta_0.wait_recv()
        corner_0.wait_recv()
        select(from_corner, 0, rows_in.at[2], meta_in.at[2])
        ffn(from_corner, 0, gate_a, up_a, down_a, 2)

    def start_late():
        late_y.start()
        by_x[6].start()
        by_core[6].start()

    def pass_late():
        late_y.wait_recv()
        late_x.start()
        late_core.start()

    def relay_late():
        late_x.wait_recv()
        late_relay.start()

    def add_passing(position, where):
        partial[position, where, :] = (
            partial[position, where, :].astype(jnp.float32) + passing[where].astype(jnp.float32)
        ).astype(jnp.bfloat16)

    def merge_z():
        pass_z.wait_recv()
        add_passing(from_y, z_part)
        back_y2.start()

    def merge_y():
        pass_y.wait_recv()
        add_passing(from_z, y_part)
        back_z2.start()

    def finish(position, parts, *copies):
        ffn(position, 1, gate_b, up_b, down_b, parts)
        gather_back(position)
        for copy in copies:
            copy.start()

    def finish_own(parts):
        ffn(own, 1, gate_b, up_b, down_b, parts)
        for which in range(2):
            start_sum(which)

    def late_hidden(position, place, copy):
        lines = activate(picked[1, position], gate_b[:, later], up_b[:, later])
        if copy is None:
            hidden_in[place] = lines
        else:
            hidden_out[place] = lines
            copy.start()

    def add_late(which):
        @pl.loop(0, 4, unroll=2)
        def _(step):
            wide = width // 4
            part = pl.ds(pl.multiple_of(step * wide, wide), wide)
            values[halves[which], part] += jnp.dot(
                late_spread[which], late_rows[which, :, part], preferred_element_type=jnp.float32
            )

    def late_result(place, down):
        @pl.loop(0, 4, unroll=2)
        def _(step):
            wide = width // 4
            part = pl.ds(pl.multiple_of(step * wide, wide), wide)
            result = jnp.dot(hidden_in[place], down[:, part], preferred_element_type=jnp.float32)
            result = (result * late_weight[place]).astype(jnp.bfloat16)
            for which in range(2):
                late_rows[which, pl.ds(place * slots, slots), part] = result[
                    which * slots : (which + 1) * slots
                ]

    @pl.when(outer)
    def _():
        pass_far(0)
        pass_far(1)
        take_y1()
        pass_far(2)
        pass_x(0)
        pass_x(1)
        take_z1()
        pass_x(2)
        take_y0()
        settle((0, 1, 2))
        take_z0()
        finish(from_z, 1)
        far[6].wait_recv()
        late_z.start()
        start_late()
        finish(from_y, 1, back_y1)
        take_corner1()
        pass_x(6)
        take_corner0()
        start_far((3, 4), outer)
        back_z1.start()
        finish(from_corner, 1, pass_y, pass_z)
        finish_own(1)
        pass_late()
        pass_far(3)
        relay_late()
        pass_far(4)
        pass_x(3)
        merge_z()
        pass_x(4)
        settle((3, 4))
        late_hidden(from_corner, 2, hidden_corner)
        late_hidden(from_y, 0, hidden_y)
        late_hidden(from_z, 1, hidden_z)
        merge_y()
        late_hidden(own, 0, None)
        settle((6,))
        late_core.wait_recv()
        late_relay.wait_recv()
        late_result(0, late_a)
        hidden_y.wait_recv()

    @pl.when(inner)
    def _():
        take_y1()
        pass_far(0)
        take_z1()
        pass_far(1)
        pass_x(0)
        take_y0()
        pass_far(2)
        pass_x(1)
        take_z0()
        pass_far(3)
        pass_x(2)
        pass_far(4)
        pass_x(3)
        take_corner1()
        pass_far(5)
        pass_x(4)
        take_corner0()
        late_z.wait_recv()
        start_late()
        pass_x(5)
        settle((0, 1, 2, 3, 4, 5))
        finish(from_corner, 2, pass_y, pass_z)
        finish(from_y, 2, back_y1)
        finish(from_z, 2, back_z1)
        pass_x(6)
        finish_own(2)
        pass_late()
        merge_z()
        relay_late()
        merge_y()
        settle((6,))
        late_core.wait_recv()
        late_relay.wait_recv()
        hidden_z.wait_recv()
        late_result(0, late_a)
        hidden_corner.wait_recv()

    late_result(1, late_b)
    for which in range(2):
        add_late(which)
    for copy in ends:
        copy.wait()
    for copy in (back_y1, back_z1, back_y2, back_z2):
        copy.wait_recv()

    @pl.loop(0, rows // 16, unroll=2)
    def _(step):
        part = pl.ds(pl.multiple_of(step * 16, 16), 16)
        total = values[part, :] + arrived[0, part, :].astype(jnp.float32)
        total = total + arrived[1, part, :].astype(jnp.float32)
        out[part, :] = layer_norm(total, gain[...], shift[...]).astype(jnp.bfloat16)

    for copy, when in made:
        if when is None:
            copy.wait_send()
        else:
            pl.when(when)(copy.wait_send)


def near_layer(
    residual,
    pool_input,
    doc_ids,
    pool_map,
    pool_scale,
    out_weight,
    mix_gain,
    mix_shift,
    group_router,
    expert_router,
    expert_gate,
    expert_up,
    expert_down,
    routes,
    ffn_gain,
    ffn_shift,
):
    expert_count = lax.axis_size("sp")
    rows, width = residual.shape
    ff = expert_gate.shape[2]
    seq_rows, group_width = pool_input.shape
    pool_width = out_weight.shape[0]
    group_count = group_router.shape[1]
    half = rows // 2
    slots = half * routes.shape[1] * 2 // expert_count
    anywhere = pl.BlockSpec(memory_space=pl.ANY)
    bf16, f32 = jnp.bfloat16, jnp.float32
    operands = (
        residual,
        pool_input,
        doc_ids.reshape(seq_rows // block, block),
        pool_map,
        pool_scale[None, :],
        out_weight,
        mix_gain[None, :],
        mix_shift[None, :],
        group_router.T,
        expert_router.T,
        routes.T,
        expert_gate,
        expert_up,
        expert_down,
        ffn_gain[None, :],
        ffn_shift[None, :],
    )
    return pl.pallas_call(
        functools.partial(layer_kernel, (slots, expert_count)),
        out_shape=jax.ShapeDtypeStruct((rows, width), bf16),
        in_specs=[anywhere] * len(operands),
        out_specs=pl.BlockSpec(memory_space=pltpu.VMEM),
        scratch_shapes=[
            pltpu.VMEM((rows, width), bf16),
            pltpu.VMEM((seq_rows + block, group_width), bf16),
            pltpu.VMEM((16, block), jnp.int32),
            pltpu.VMEM((group_width, group_width), bf16),
            pltpu.VMEM((1, group_width), f32),
            pltpu.VMEM((pool_width, width), bf16),
            pltpu.VMEM((1, width), f32),
            pltpu.VMEM((1, width), f32),
            pltpu.VMEM((group_count, width), bf16),
            pltpu.VMEM((expert_count, width), bf16),
            pltpu.VMEM(routes.shape[::-1], jnp.int32),
            pltpu.VMEM((1, width), f32),
            pltpu.VMEM((1, width), f32),
            pltpu.VMEM((6, block, group_width), bf16),
            pltpu.VMEM((2, half, pool_width), bf16),
            pltpu.VMEM((rows, width), f32),
            pltpu.VMEM((rows, width), bf16),
            pltpu.VMEM((2, 2 * expert_count, half), f32),
            pltpu.VMEM((width, ff), bf16),
            pltpu.VMEM((width, ff), bf16),
            pltpu.VMEM((ff, width), bf16),
            pltpu.VMEM((width, ff), bf16),
            pltpu.VMEM((width, ff), bf16),
            pltpu.VMEM((ff, width), bf16),
            pltpu.VMEM((3, rows, width), bf16),
            pltpu.VMEM((3, 2, 2 * expert_count, half), f32),
            pltpu.VMEM((2, 4, 2 * slots, width), bf16),
            pltpu.VMEM((4, 2, half, 2 * slots), bf16),
            pltpu.VMEM((2, 4, 2 * slots, 1), f32),
            pltpu.VMEM((2 * slots, ff), bf16),
            pltpu.VMEM((4, 2, 2 * slots, width), bf16),
            pltpu.VMEM((3, rows, width), bf16),
            pltpu.VMEM((rows, width), bf16),
            pltpu.VMEM((2, rows, width), bf16),
            pltpu.VMEM((3, 2 * slots, ff // 2), bf16),
            pltpu.VMEM((2, 2 * slots, ff // 2), bf16),
            pltpu.VMEM((ff // 2, width), bf16),
            pltpu.VMEM((ff // 2, width), bf16),
            pltpu.VMEM((2, half, 2 * slots), bf16),
            pltpu.VMEM((2, 2 * slots, 1), f32),
            pltpu.VMEM((2, 2 * slots, width), bf16),
            pltpu.SemaphoreType.DMA((16,)),
            pltpu.SemaphoreType.DMA((80,)),
            pltpu.SemaphoreType.DMA((80,)),
        ],
        compiler_params=pltpu.CompilerParams(
            collective_id=0, has_side_effects=True, vmem_limit_bytes=60 * 1024 * 1024
        ),
    )(*operands)


def on_device(
    residual,
    pool_input,
    doc_ids,
    pool_map,
    pool_scale,
    out_weight,
    mix_gain,
    mix_shift,
    group_router,
    expert_router,
    expert_gate,
    expert_up,
    expert_down,
    routes,
    ffn_gain,
    ffn_shift,
):
    seq_rows = pool_input.shape[0]
    reach_rows = 15
    expert_count = lax.axis_size("sp")
    tp_count = lax.axis_size("tp")
    near = expert_count == 2 * group_size and tp_count == group_size
    near = near and residual.shape[0] == 2 * block and seq_rows == tp_count * residual.shape[0]
    if near:
        return near_layer(
            residual,
            pool_input,
            doc_ids,
            pool_map,
            pool_scale,
            out_weight,
            mix_gain,
            mix_shift,
            group_router,
            expert_router,
            expert_gate,
            expert_up,
            expert_down,
            routes,
            ffn_gain,
            ffn_shift,
        )
    window = jnp.left_shift(jnp.int32(2), lax.axis_index("tp"))
    first_row = lax.axis_index("sp") * seq_rows
    tail_values, tail_docs = from_behind(
        (pool_input[seq_rows - reach_rows :], doc_ids[seq_rows - reach_rows :]), "sp", 1
    )
    source = jnp.concatenate([tail_values, pool_input], axis=0).astype(jnp.float32)
    all_docs = jnp.concatenate([tail_docs, doc_ids], axis=0)
    positions = first_row - reach_rows + jnp.arange(seq_rows + reach_rows, dtype=jnp.int32)
    running = jnp.zeros((seq_rows, source.shape[1]), jnp.float32)
    weight_sum = jnp.zeros((seq_rows, 1), jnp.float32)
    for offset in range(reach_rows + 1):
        begin_row = reach_rows - offset
        earlier = source[begin_row : begin_row + seq_rows]
        keep_mask = (
            (all_docs[begin_row : begin_row + seq_rows] == doc_ids)
            & (positions[begin_row : begin_row + seq_rows] >= 0)
            & (offset < window)
        )
        same_doc = keep_mask.astype(jnp.float32)[:, None]
        running = running + same_doc * earlier
        weight_sum = weight_sum + same_doc
    pooled = (running / weight_sum - source[reach_rows:]).astype(jnp.bfloat16)
    mixed = (jnp.dot(pooled, pool_map[0], preferred_element_type=jnp.float32) * pool_scale).astype(
        jnp.bfloat16
    )
    row_count = seq_rows // tp_count
    blocks = mixed.reshape(tp_count, row_count, mixed.shape[1])
    branch = jnp.einsum(
        "abc,cd->abd",
        lax.all_to_all(blocks, "tp", split_axis=0, concat_axis=2, tiled=True),
        out_weight,
        preferred_element_type=jnp.float32,
    )[0]
    normed = layer_norm(
        skip_scale * residual.astype(jnp.float32) + branch, mix_gain, mix_shift
    ).astype(jnp.bfloat16)
    weight = route_weights(normed, routes, group_router, expert_router)
    half_most = row_count * routes.shape[1] // expert_count
    half_rows = row_count // 2
    routed_parts = []
    for piece_index in range(2):
        rows_here = slice(piece_index * half_rows, (piece_index + 1) * half_rows)
        outgoing, slot_index = fill_slots(
            normed[rows_here], routes[rows_here], half_most, expert_count
        )
        returned = lax.all_to_all(
            expert_ffn(
                lax.all_to_all(outgoing, "sp", split_axis=0, concat_axis=0, tiled=True),
                expert_gate,
                expert_up,
                expert_down,
            ),
            "sp",
            split_axis=0,
            concat_axis=0,
            tiled=True,
        )
        routed_parts.append(combine_rows(returned, slot_index, weight[rows_here]))
    routed = jnp.concatenate(routed_parts, axis=0)
    return layer_norm(skip_scale * normed.astype(jnp.float32) + routed, ffn_gain, ffn_shift).astype(
        jnp.bfloat16
    )


def solution(mesh):
    in_specs = (
        P(("sp", "tp"), None),
        P("sp", "tp"),
        P("sp"),
        P("tp", None, None),
        P("tp"),
        P(),
        P(),
        P(),
        P(),
        P(),
        P("sp", None, None),
        P("sp", None, None),
        P("sp", None, None),
        P(("sp", "tp"), None),
        P(),
        P(),
    )
    out_specs = P(("sp", "tp"), None)
    return jax.shard_map(
        on_device, mesh=mesh, in_specs=in_specs, out_specs=out_specs, check_vma=False
    )
```

```python
import functools

import jax
import jax.numpy as jnp
from jax import lax
from jax.experimental import pallas as pl
from jax.experimental.pallas import tpu as pltpu
from jax.sharding import PartitionSpec as P

skip_scale = 2.0**0.5
epsilon = 1e-05


def from_behind(block, axis, distance):
    devices = range(lax.axis_size(axis))
    route = [(i - distance, i) for i in devices if i - distance in devices]
    return lax.ppermute(block, axis, route)


def layer_norm(values, norm_gain, norm_shift):
    center = values - jnp.mean(values, axis=-1, keepdims=True)
    spread = jnp.mean(center * center, axis=-1, keepdims=True)
    return center * lax.rsqrt(spread + epsilon) * norm_gain + norm_shift


def route_weights(normed, chosen, group_router, expert_router):
    group_logits = jnp.dot(normed, group_router, preferred_element_type=jnp.float32)
    expert_logits = jnp.dot(normed, expert_router, preferred_element_type=jnp.float32)
    group_count = group_logits.shape[1]
    expert_count = expert_logits.shape[1]
    group_exp = jnp.exp(group_logits)
    group_prob = group_exp / jnp.sum(group_exp, axis=1, keepdims=True)
    expert_ids = jnp.arange(expert_count, dtype=jnp.int32)
    picked = jnp.sum(
        jnp.where(chosen[:, :, None] == expert_ids[None, None, :], expert_logits[:, None, :], 0.0),
        axis=2,
    )
    picked_exp = jnp.exp(picked)
    pair_share = picked_exp / jnp.sum(picked_exp, axis=1, keepdims=True)
    group_of = chosen // (expert_count // group_count)
    group_ids = jnp.arange(group_count, dtype=jnp.int32)
    group_share = jnp.sum(
        jnp.where(group_of[:, :, None] == group_ids[None, None, :], group_prob[:, None, :], 0.0),
        axis=2,
    )
    return group_share * pair_share


def expert_ffn(arrived, expert_gate, expert_up, expert_down):
    sources, slot_count, width = arrived.shape
    gathered = arrived.reshape(sources * slot_count, width)
    gate_out = jnp.dot(gathered, expert_gate[0], preferred_element_type=jnp.float32)
    up_out = jnp.dot(gathered, expert_up[0], preferred_element_type=jnp.float32)
    hidden = (jax.nn.silu(gate_out) * up_out).astype(jnp.bfloat16)
    result = jnp.dot(hidden, expert_down[0], preferred_element_type=jnp.float32).astype(
        jnp.bfloat16
    )
    return result.reshape(sources, slot_count, width)


def fill_slots(normed, chosen, capacity, expert_count):
    flat_routes = chosen.reshape(-1)
    entry_count = flat_routes.shape[0]
    onehot = (flat_routes[:, None] == jnp.arange(expert_count, dtype=jnp.int32)[None, :]).astype(
        jnp.int32
    )
    slot_rank = jnp.sum((jnp.cumsum(onehot, axis=0) - onehot) * onehot, axis=1)
    slot_index = flat_routes * capacity + slot_rank
    token_ids = jnp.arange(entry_count, dtype=jnp.int32) // chosen.shape[1]
    source_row = (
        jnp.full((expert_count * capacity,), normed.shape[0], jnp.int32)
        .at[slot_index]
        .set(token_ids)
    )
    padded = jnp.concatenate([normed, jnp.zeros((1, normed.shape[1]), normed.dtype)], axis=0)
    outgoing = jnp.take(padded, source_row, axis=0).reshape(expert_count, capacity, normed.shape[1])
    return (outgoing, slot_index)


def combine_rows(returned, slot_index, weight):
    flat_out = returned.reshape(-1, returned.shape[2])
    picked = jnp.take(flat_out, slot_index, axis=0).reshape(
        weight.shape[0], weight.shape[1], flat_out.shape[1]
    )
    return jnp.sum(weight[:, :, None] * picked.astype(jnp.float32), axis=1)


MESH = pl.DeviceIdType.MESH
group_size = 4
block = 128


def flip(index, bit):
    return index + bit - 2 * bit * ((index // bit) % 2)


def opposite(index):
    return flip(flip(index, 2), group_size)


def layer_kernel(
    dims,
    residual_hbm,
    pool_hbm,
    docs_hbm,
    map_hbm,
    scale_hbm,
    weight_hbm,
    mix_gain_hbm,
    mix_shift_hbm,
    group_router_hbm,
    expert_router_hbm,
    routes_hbm,
    own_gate,
    own_up,
    own_down,
    gain_hbm,
    shift_hbm,
    out,
    residual,
    source,
    docs,
    pool_map,
    pool_scale,
    out_weight,
    mix_gain,
    mix_shift,
    group_router,
    expert_router,
    routes,
    gain,
    shift,
    mixed_out,
    mixed_in,
    values,
    normed,
    meta,
    gate_a,
    up_a,
    down_a,
    gate_b,
    up_b,
    down_b,
    rows_in,
    meta_in,
    picked,
    spread,
    slot_weight,
    hidden,
    weighted,
    partial,
    passing,
    arrived,
    hidden_out,
    hidden_in,
    late_a,
    late_b,
    late_spread,
    late_weight,
    late_rows,
    load_sems,
    send_sems,
    recv_sems,
):
    slots, expert_count = dims
    rows, width = normed.shape
    half = rows // 2
    ff = own_gate.shape[2]
    seq_rows, group_width = pool_hbm.shape
    reach = 16
    outer_y, inner_y = rows * 13 // 16, rows // 2
    sp, tp = lax.axis_index("sp"), lax.axis_index("tp")
    sp_count = expert_count
    to_y = {"sp": flip(sp, 1)}
    to_z = {"sp": flip(sp, 2)}
    to_far = {"sp": opposite(sp)}
    to_next = {"sp": (sp + 1) % sp_count}
    to_last = {"sp": (sp + sp_count - 1) % sp_count}
    to_x = {"tp": flip(tp, 2)}
    to_core = {"tp": flip(tp, 1)}
    to_corner = {"sp": flip(flip(sp, 1), 2)}
    to_diag = {"tp": flip(flip(tp, 2), 1)}
    inner = ((sp // 2 + 1) // 2) % 2 == 1

    barrier = pltpu.get_barrier_semaphore()
    peers = (to_y, to_z, to_corner, to_far, to_next, to_last, to_x, to_core, to_diag)
    for peer in peers:
        pl.semaphore_signal(barrier, inc=1, device_id=peer, device_id_type=MESH)

    loads = []

    def load(src, dst):
        copy = pltpu.make_async_copy(src, dst, load_sems.at[len(loads)])
        copy.start()
        loads.append(copy)
        return copy

    load_source = load(pool_hbm, source.at[pl.ds(block, seq_rows)])
    load_docs = load(docs_hbm, docs.at[pl.ds(8, 8)])
    load_map = load(map_hbm.at[0], pool_map)
    load_scale = load(scale_hbm, pool_scale)
    front = [
        load(residual_hbm, residual),
        load(weight_hbm, out_weight),
        load(mix_gain_hbm, mix_gain),
        load(mix_shift_hbm, mix_shift),
        load(group_router_hbm, group_router),
        load(expert_router_hbm, expert_router),
        load(routes_hbm, routes),
    ]
    experts_in = [
        load(own_gate.at[0], gate_a),
        load(own_up.at[0], up_a),
        load(own_down.at[0], down_a),
    ]
    ends = [load(gain_hbm, gain), load(shift_hbm, shift)]

    source[pl.ds(0, block - reach), :] = jnp.zeros((block - reach, group_width), jnp.bfloat16)
    pl.semaphore_wait(barrier, len(peers))

    made = []

    def send(src, dst, peer, when=None, start=True):
        index = len(made)
        copy = pltpu.make_async_remote_copy(
            src_ref=src,
            dst_ref=dst,
            send_sem=send_sems.at[index],
            recv_sem=recv_sems.at[index],
            device_id=peer,
            device_id_type=MESH,
        )
        made.append((copy, when))
        if start and when is None:
            copy.start()
        elif start:
            pl.when(when)(copy.start)
        return copy

    tail_rows = send(
        pool_hbm.at[pl.ds(seq_rows - reach, reach)], source.at[pl.ds(block - reach, reach)], to_next
    )
    tail_docs = send(docs_hbm, docs.at[pl.ds(0, 8)], to_next)

    quarter = width // 4
    late = ff // 2

    def share(position):
        return pl.ds(pl.multiple_of(position * quarter, quarter), quarter)

    mine, across = share(tp), share(flip(tp, 2))
    soon, later = pl.ds(0, late), pl.ds(late, late)
    outer = jnp.logical_not(inner)
    chunks = [
        (own_gate.at[0, mine, soon], gate_b.at[mine, soon], gate_b.at[across, soon], None),
        (own_up.at[0, mine, soon], up_b.at[mine, soon], up_b.at[across, soon], None),
        (own_down.at[0, soon, mine], down_b.at[soon, mine], down_b.at[soon, across], None),
        (own_gate.at[0, mine, later], gate_b.at[mine, later], gate_b.at[across, later], None),
        (own_up.at[0, mine, later], up_b.at[mine, later], up_b.at[across, later], None),
        (own_down.at[0, later, mine], down_b.at[later, mine], down_b.at[later, across], inner),
        (own_down.at[0, later, mine], late_a.at[:, mine], late_a.at[:, across], outer),
    ]
    far = [
        send(own_part, kept, to_far, when, start=False)
        for own_part, kept, beside, when in chunks
    ]
    by_x = [
        send(kept, kept, to_x, inner if when is inner else None, start=False)
        for own_part, kept, beside, when in chunks
    ]
    by_core = [
        send(kept, kept, to_core, inner if when is inner else None, start=False)
        for own_part, kept, beside, when in chunks
    ]
    by_relay = [
        send(beside, beside, to_core, inner if when is inner else None, start=False)
        for own_part, kept, beside, when in chunks
    ]

    def start_far(indices, when):
        @pl.when(when)
        def _():
            for index in indices:
                far[index].start()

    start_far((0, 1, 2), outer)
    start_far((0, 1, 2, 3, 4, 5), inner)

    window = 2 * (1 + tp % 2) * (1 + 3 * (tp // 2))
    row_ids = lax.broadcasted_iota(jnp.int32, (block, 2 * block), 0)
    col_ids = lax.broadcasted_iota(jnp.int32, (block, 2 * block), 1)
    behind = row_ids + block - col_ids
    in_window = (behind >= 0) & (behind < window)
    first, second = pl.ds(0, half), pl.ds(half, half)
    halves = (first, second)
    destinations = (
        (flip(tp, 2), to_x),
        (flip(flip(tp, 2), 1), to_diag),
        (flip(tp, 1), to_core),
        (tp, None),
    )
    channels = pl.ds(pl.multiple_of(tp * group_width, group_width), group_width)
    load_source.wait()
    load_docs.wait()
    load_map.wait()
    load_scale.wait()

    mixed_sent = {0: [], 1: []}

    def mix(which):
        for owner, peer in destinations:
            index = owner * 2 + which
            start = pl.multiple_of(index * block, block)
            here = docs[pl.ds(index + 8, 1), :].astype(jnp.float32)
            before = docs[pl.ds(index + 7, 1), :].astype(jnp.float32)
            across_docs = jnp.concatenate([before, here], axis=1)
            down_docs = jnp.transpose(jnp.broadcast_to(here, (block, block)))
            down_docs = jnp.concatenate([down_docs, down_docs], axis=1)
            known = col_ids + (sp * seq_rows + start) >= block
            keep = jnp.where(in_window & known & (across_docs == down_docs), 1.0, 0.0)
            total = jnp.dot(
                keep.astype(jnp.bfloat16),
                source[pl.ds(start, 2 * block), :],
                preferred_element_type=jnp.float32,
            )
            count = jnp.sum(keep, axis=1, keepdims=True)
            center = source[pl.ds(start + block, block), :].astype(jnp.float32)
            pooled = (total / count - center).astype(jnp.bfloat16)
            mixed = jnp.dot(pooled, pool_map[...], preferred_element_type=jnp.float32)
            mixed = (mixed * pool_scale[...]).astype(jnp.bfloat16)
            if peer is None:
                mixed_in[which, :, channels] = mixed
            else:
                place = len(mixed_sent[0]) + len(mixed_sent[1])
                mixed_out[place] = mixed
                mixed_sent[which].append(
                    send(mixed_out.at[place], mixed_in.at[which, :, channels], peer)
                )

    mix(1)
    tail_rows.wait_recv()
    tail_docs.wait_recv()
    mix(0)

    slot_cols = lax.broadcasted_iota(jnp.int32, (half, half), 1)
    slot_rows = lax.broadcasted_iota(jnp.int32, (half, half), 0)
    earlier = jnp.where(slot_rows < slot_cols, 1.0, 0.0).astype(jnp.bfloat16)
    expert_ids = lax.broadcasted_iota(jnp.int32, (expert_count, half), 0)
    group_count = group_router.shape[0]
    transposed = (((1,), (1,)), ((), ()))

    def project(which):
        where = halves[which]
        for copy in mixed_sent[which]:
            copy.wait_recv()

        @pl.loop(0, 4, unroll=2)
        def _(step):
            wide = width // 4
            part = pl.ds(pl.multiple_of(step * wide, wide), wide)
            values[where, part] = skip_scale * residual[where, part].astype(jnp.float32) + jnp.dot(
                mixed_in[which], out_weight[:, part], preferred_element_type=jnp.float32
            )

        @pl.loop(0, half // 16, unroll=2)
        def _(step):
            part = pl.ds(pl.multiple_of(which * half + step * 16, 16), 16)
            normed[part, :] = layer_norm(values[part, :], mix_gain[...], mix_shift[...]).astype(
                jnp.bfloat16
            )

    def route(which):
        where = halves[which]
        lines = normed[where, :]
        group_logits = lax.dot_general(
            group_router[...], lines, transposed, preferred_element_type=jnp.float32
        )
        expert_logits = lax.dot_general(
            expert_router[...], lines, transposed, preferred_element_type=jnp.float32
        )
        group_exp = jnp.exp(group_logits)
        group_prob = group_exp / jnp.sum(group_exp, axis=0, keepdims=True)
        named = (routes[0:1, where] == expert_ids) | (routes[1:2, where] == expert_ids)
        group_share = jnp.zeros((expert_count, half), jnp.float32)
        for group in range(group_count):
            group_share = jnp.where(
                expert_ids // (expert_count // group_count) == group,
                group_prob[group : group + 1, :],
                group_share,
            )
        picked_exp = jnp.where(named, jnp.exp(jnp.where(named, expert_logits, 0.0)), 0.0)
        share = group_share * (picked_exp / jnp.sum(picked_exp, axis=0, keepdims=True))
        ones = jnp.where(named, 1.0, 0.0)
        rank = jnp.dot(ones.astype(jnp.bfloat16), earlier, preferred_element_type=jnp.float32)
        meta[which, pl.ds(0, expert_count), :] = jnp.where(named, rank, -1.0)
        meta[which, pl.ds(expert_count, expert_count), :] = share

    for copy in front:
        copy.wait()
    rows_y, rows_z, meta_y, meta_z = {}, {}, {}, {}
    for which in (1, 0):
        where = halves[which]
        project(which)
        route(which)
        meta_y[which] = send(meta.at[which], meta_in.at[0, which], to_y)
        meta_z[which] = send(meta.at[which], meta_in.at[1, which], to_z)
        rows_y[which] = send(normed.at[where], rows_in.at[0, where], to_y)
        rows_z[which] = send(normed.at[where], rows_in.at[1, where], to_z)

    start_far((6,), outer)

    slot_ids = lax.broadcasted_iota(jnp.int32, (slots, half), 0).astype(jnp.float32)
    experts = (sp, opposite(sp))

    def select(position, which, row_ref, meta_ref):
        parts = []
        for kind in range(2):
            slot_row = meta_ref[which, pl.ds(experts[kind], 1), :]
            weight_row = meta_ref[which, pl.ds(expert_count + experts[kind], 1), :]
            match = jnp.where(slot_ids == slot_row, 1.0, 0.0)
            slot_weight[kind, position, pl.ds(which * slots, slots), :] = jnp.sum(
                match * weight_row, axis=1, keepdims=True
            )
            parts.append(match)
        match = jnp.concatenate(parts, axis=0)
        spread[position, which] = jnp.transpose(match).astype(jnp.bfloat16)
        match = match.astype(jnp.bfloat16)

        @pl.loop(0, 4, unroll=2)
        def _(step):
            wide = width // 4
            part = pl.ds(pl.multiple_of(step * wide, wide), wide)
            found = jnp.dot(
                match, row_ref[halves[which], part], preferred_element_type=jnp.float32
            ).astype(jnp.bfloat16)
            for kind in range(2):
                picked[kind, position, pl.ds(which * slots, slots), part] = found[
                    kind * slots : (kind + 1) * slots
                ]

    def activate(lines, gate, up):
        gate_out = jnp.dot(lines, gate, preferred_element_type=jnp.float32)
        up_out = jnp.dot(lines, up, preferred_element_type=jnp.float32)
        return (gate_out / (1.0 + jnp.exp(-gate_out)) * up_out).astype(jnp.bfloat16)

    def ffn(position, kind, gate, up, down, parts):
        depth = parts * late

        @pl.loop(0, parts)
        def _(step):
            part = pl.ds(pl.multiple_of(step * late, late), late)
            hidden[:, part] = activate(picked[kind, position], gate[:, part], up[:, part])

        @pl.loop(0, 4, unroll=2)
        def _(step):
            wide = width // 4
            part = pl.ds(pl.multiple_of(step * wide, wide), wide)
            result = jnp.dot(
                hidden[:, :depth], down[:depth, part], preferred_element_type=jnp.float32
            )
            result = (result * slot_weight[kind, position]).astype(jnp.bfloat16)
            for which in range(2):
                weighted[position, which, pl.ds(kind * slots, slots), part] = result[
                    which * slots : (which + 1) * slots
                ]

    own, from_y, from_z, from_corner = 3, 0, 1, 2

    def gather_back(position):
        for which in range(2):

            @pl.loop(0, 4, unroll=2)
            def _(step):
                wide = width // 4
                part = pl.ds(pl.multiple_of(step * wide, wide), wide)
                partial[position, halves[which], part] = jnp.dot(
                    spread[position, which],
                    weighted[position, which, :, part],
                    preferred_element_type=jnp.float32,
                ).astype(jnp.bfloat16)

    def start_sum(which):
        where = halves[which]

        @pl.loop(0, 4, unroll=2)
        def _(step):
            wide = width // 4
            part = pl.ds(pl.multiple_of(step * wide, wide), wide)
            values[where, part] = skip_scale * normed[where, part].astype(jnp.float32) + jnp.dot(
                spread[own, which], weighted[own, which, :, part], preferred_element_type=jnp.float32
            )

    def pass_far(index):
        far[index].wait_recv()
        by_x[index].start()
        by_core[index].start()

    def pass_x(index):
        by_x[index].wait_recv()
        by_relay[index].start()

    def settle(indices):
        for index in indices:
            by_core[index].wait_recv()
            by_relay[index].wait_recv()

    outermost = jnp.where(inner, flip(sp, 2), sp)
    keepers = (outermost, flip(outermost, 1))
    for which in range(2):
        parts = []
        for place, keeper in enumerate(keepers):
            expert = opposite(keeper)
            match = jnp.where(slot_ids == meta[which, pl.ds(expert, 1), :], 1.0, 0.0)
            late_weight[place, pl.ds(which * slots, slots), :] = jnp.sum(
                match * meta[which, pl.ds(expert_count + expert, 1), :], axis=1, keepdims=True
            )
            parts.append(match)
        late_spread[which] = jnp.transpose(jnp.concatenate(parts, axis=0)).astype(jnp.bfloat16)

    select(own, 1, normed, meta)
    select(own, 0, normed, meta)
    for copy in experts_in:
        copy.wait()
    ffn(own, 0, gate_a, up_a, down_a, 2)

    corner_meta_1 = send(meta_in.at[0, 1], meta_in.at[2, 1], to_z, start=False)
    corner_meta_0 = send(meta_in.at[1, 0], meta_in.at[2, 0], to_y, start=False)
    corner_1 = send(rows_in.at[1, second], rows_in.at[2, second], to_y, start=False)
    corner_0 = send(rows_in.at[1, first], rows_in.at[2, first], to_y, start=False)
    late_z = send(late_a.at[:, mine], late_a.at[:, mine], to_z, outer, start=False)
    late_y = send(late_a.at[:, mine], late_b.at[:, mine], to_y, start=False)
    late_x = send(late_b.at[:, mine], late_b.at[:, mine], to_x, start=False)
    late_core = send(late_b.at[:, mine], late_b.at[:, mine], to_core, start=False)
    late_relay = send(late_b.at[:, across], late_b.at[:, across], to_core, start=False)

    def split(count):
        return pl.ds(0, count), pl.ds(count, rows - count)

    def results(plane, mine_y, other_y):
        def move(position, where, place, slot, peer):
            return send(
                partial.at[position, where], place.at[slot, where], peer, plane, start=False
            )

        y_part, z_part = split(mine_y)
        first_part, last_part = split(other_y)
        return (
            move(from_corner, y_part, passing, 0, to_y),
            move(from_corner, z_part, passing, 1, to_z),
            move(from_y, first_part, arrived, 0, to_y),
            move(from_y, last_part, arrived, 0, to_y),
            move(from_z, z_part, arrived, 1, to_z),
            move(from_z, y_part, arrived, 1, to_z),
        )

    outer_results = results(outer, outer_y, inner_y)
    inner_results = results(inner, inner_y, outer_y)
    hidden_y = send(hidden_out.at[0], hidden_in.at[1], to_y, outer, start=False)
    hidden_z = send(hidden_out.at[1], hidden_in.at[0], to_z, outer, start=False)
    hidden_corner = send(hidden_out.at[2], hidden_in.at[1], to_corner, outer, start=False)

    def take_y1():
        meta_y[1].wait_recv()
        corner_meta_1.start()
        rows_y[1].wait_recv()
        select(from_y, 1, rows_in.at[0], meta_in.at[0])

    def take_y0():
        meta_y[0].wait_recv()
        rows_y[0].wait_recv()
        select(from_y, 0, rows_in.at[0], meta_in.at[0])
        ffn(from_y, 0, gate_a, up_a, down_a, 2)

    def take_z1():
        meta_z[1].wait_recv()
        rows_z[1].wait_recv()
        corner_1.start()
        select(from_z, 1, rows_in.at[1], meta_in.at[1])

    def take_z0():
        meta_z[0].wait_recv()
        corner_meta_0.start()
        rows_z[0].wait_recv()
        corner_0.start()
        select(from_z, 0, rows_in.at[1], meta_in.at[1])
        ffn(from_z, 0, gate_a, up_a, down_a, 2)

    def take_corner1():
        corner_meta_1.wait_recv()
        corner_1.wait_recv()
        select(from_corner, 1, rows_in.at[2], meta_in.at[2])

    def take_corner0():
        corner_meta_0.wait_recv()
        corner_0.wait_recv()
        select(from_corner, 0, rows_in.at[2], meta_in.at[2])
        ffn(from_corner, 0, gate_a, up_a, down_a, 2)

    def start_late():
        late_y.start()
        by_x[6].start()
        by_core[6].start()

    def pass_late():
        late_y.wait_recv()
        late_x.start()
        late_core.start()

    def relay_late():
        late_x.wait_recv()
        late_relay.start()

    def add_passing(position, where, slot):
        partial[position, where, :] = (
            partial[position, where, :].astype(jnp.float32)
            + passing[slot, where, :].astype(jnp.float32)
        ).astype(jnp.bfloat16)

    def merge_z(here, there, other_y):
        there[1].wait_recv()
        add_passing(from_y, split(other_y)[1], 1)
        here[3].start()

    def merge_y(here, mine_y):
        here[0].wait_recv()
        add_passing(from_z, split(mine_y)[0], 0)
        here[5].start()

    def finish(position, parts, *copies):
        ffn(position, 1, gate_b, up_b, down_b, parts)
        gather_back(position)
        for copy in copies:
            copy.start()

    def finish_own(parts):
        ffn(own, 1, gate_b, up_b, down_b, parts)
        for which in range(2):
            start_sum(which)

    def late_hidden(position, place, copy):
        lines = activate(picked[1, position], gate_b[:, later], up_b[:, later])
        if copy is None:
            hidden_in[place] = lines
        else:
            hidden_out[place] = lines
            copy.start()

    def add_late(which):
        @pl.loop(0, 4, unroll=2)
        def _(step):
            wide = width // 4
            part = pl.ds(pl.multiple_of(step * wide, wide), wide)
            values[halves[which], part] += jnp.dot(
                late_spread[which], late_rows[which, :, part], preferred_element_type=jnp.float32
            )

    def late_result(place, down):
        @pl.loop(0, 4, unroll=2)
        def _(step):
            wide = width // 4
            part = pl.ds(pl.multiple_of(step * wide, wide), wide)
            result = jnp.dot(hidden_in[place], down[:, part], preferred_element_type=jnp.float32)
            result = (result * late_weight[place]).astype(jnp.bfloat16)
            for which in range(2):
                late_rows[which, pl.ds(place * slots, slots), part] = result[
                    which * slots : (which + 1) * slots
                ]

    @pl.when(outer)
    def _():
        pass_y, pass_z, back_y1, back_y2, back_z1, back_z2 = outer_results
        pass_far(0)
        pass_far(1)
        take_y1()
        pass_far(2)
        pass_x(0)
        pass_x(1)
        take_z1()
        pass_x(2)
        take_y0()
        settle((0, 1, 2))
        take_z0()
        finish(from_z, 1)
        far[6].wait_recv()
        late_z.start()
        start_late()
        back_z1.start()
        finish(from_y, 1)
        take_corner1()
        pass_x(6)
        take_corner0()
        start_far((3, 4), outer)
        finish(from_corner, 1, pass_y, pass_z, back_y1)
        finish_own(1)
        pass_late()
        pass_far(3)
        relay_late()
        pass_far(4)
        pass_x(3)
        pass_x(4)
        settle((3, 4))
        late_hidden(from_corner, 2, hidden_corner)
        late_hidden(from_y, 0, hidden_y)
        late_hidden(from_z, 1, hidden_z)
        merge_y(outer_results, outer_y)
        merge_z(outer_results, inner_results, inner_y)
        late_hidden(own, 0, None)
        settle((6,))
        late_core.wait_recv()
        late_relay.wait_recv()
        late_result(0, late_a)
        hidden_y.wait_recv()

    @pl.when(inner)
    def _():
        pass_y, pass_z, back_y1, back_y2, back_z1, back_z2 = inner_results
        take_y1()
        pass_far(0)
        take_z1()
        pass_far(1)
        pass_x(0)
        take_y0()
        pass_far(2)
        pass_x(1)
        take_z0()
        pass_far(3)
        pass_x(2)
        pass_far(4)
        pass_x(3)
        take_corner1()
        pass_far(5)
        pass_x(4)
        take_corner0()
        late_z.wait_recv()
        late_y.start()
        pass_x(5)
        by_x[6].start()
        by_core[6].start()
        settle((0, 1, 2, 3, 4, 5))
        finish(from_corner, 2, pass_y, pass_z)
        finish(from_y, 2, back_y1)
        finish(from_z, 2, back_z1)
        pass_x(6)
        finish_own(2)
        pass_late()
        merge_y(inner_results, inner_y)
        merge_z(inner_results, outer_results, outer_y)
        relay_late()
        settle((6,))
        late_core.wait_recv()
        late_relay.wait_recv()
        hidden_z.wait_recv()
        late_result(0, late_a)
        hidden_corner.wait_recv()

    late_result(1, late_b)
    for which in range(2):
        add_late(which)
    for copy in ends:
        copy.wait()

    @pl.when(outer)
    def _():
        outer_results[2].wait_recv()
        outer_results[3].wait_recv()
        inner_results[4].wait_recv()
        inner_results[5].wait_recv()

    @pl.when(inner)
    def _():
        inner_results[2].wait_recv()
        inner_results[3].wait_recv()
        outer_results[4].wait_recv()
        outer_results[5].wait_recv()


    @pl.loop(0, rows // 16, unroll=4)
    def _(step):
        part = pl.ds(pl.multiple_of(step * 16, 16), 16)
        total = values[part, :] + arrived[0, part, :].astype(jnp.float32)
        total = total + arrived[1, part, :].astype(jnp.float32)
        out[part, :] = layer_norm(total, gain[...], shift[...]).astype(jnp.bfloat16)

    for copy, when in made:
        if when is None:
            copy.wait_send()
        else:
            pl.when(when)(copy.wait_send)


def near_layer(
    residual,
    pool_input,
    doc_ids,
    pool_map,
    pool_scale,
    out_weight,
    mix_gain,
    mix_shift,
    group_router,
    expert_router,
    expert_gate,
    expert_up,
    expert_down,
    routes,
    ffn_gain,
    ffn_shift,
):
    expert_count = lax.axis_size("sp")
    rows, width = residual.shape
    ff = expert_gate.shape[2]
    seq_rows, group_width = pool_input.shape
    pool_width = out_weight.shape[0]
    group_count = group_router.shape[1]
    half = rows // 2
    slots = half * routes.shape[1] * 2 // expert_count
    anywhere = pl.BlockSpec(memory_space=pl.ANY)
    bf16, f32 = jnp.bfloat16, jnp.float32
    operands = (
        residual,
        pool_input,
        doc_ids.reshape(seq_rows // block, block),
        pool_map,
        pool_scale[None, :],
        out_weight,
        mix_gain[None, :],
        mix_shift[None, :],
        group_router.T,
        expert_router.T,
        routes.T,
        expert_gate,
        expert_up,
        expert_down,
        ffn_gain[None, :],
        ffn_shift[None, :],
    )
    return pl.pallas_call(
        functools.partial(layer_kernel, (slots, expert_count)),
        out_shape=jax.ShapeDtypeStruct((rows, width), bf16),
        in_specs=[anywhere] * len(operands),
        out_specs=pl.BlockSpec(memory_space=pltpu.VMEM),
        scratch_shapes=[
            pltpu.VMEM((rows, width), bf16),
            pltpu.VMEM((seq_rows + block, group_width), bf16),
            pltpu.VMEM((16, block), jnp.int32),
            pltpu.VMEM((group_width, group_width), bf16),
            pltpu.VMEM((1, group_width), f32),
            pltpu.VMEM((pool_width, width), bf16),
            pltpu.VMEM((1, width), f32),
            pltpu.VMEM((1, width), f32),
            pltpu.VMEM((group_count, width), bf16),
            pltpu.VMEM((expert_count, width), bf16),
            pltpu.VMEM(routes.shape[::-1], jnp.int32),
            pltpu.VMEM((1, width), f32),
            pltpu.VMEM((1, width), f32),
            pltpu.VMEM((6, block, group_width), bf16),
            pltpu.VMEM((2, half, pool_width), bf16),
            pltpu.VMEM((rows, width), f32),
            pltpu.VMEM((rows, width), bf16),
            pltpu.VMEM((2, 2 * expert_count, half), f32),
            pltpu.VMEM((width, ff), bf16),
            pltpu.VMEM((width, ff), bf16),
            pltpu.VMEM((ff, width), bf16),
            pltpu.VMEM((width, ff), bf16),
            pltpu.VMEM((width, ff), bf16),
            pltpu.VMEM((ff, width), bf16),
            pltpu.VMEM((3, rows, width), bf16),
            pltpu.VMEM((3, 2, 2 * expert_count, half), f32),
            pltpu.VMEM((2, 4, 2 * slots, width), bf16),
            pltpu.VMEM((4, 2, half, 2 * slots), bf16),
            pltpu.VMEM((2, 4, 2 * slots, 1), f32),
            pltpu.VMEM((2 * slots, ff), bf16),
            pltpu.VMEM((4, 2, 2 * slots, width), bf16),
            pltpu.VMEM((3, rows, width), bf16),
            pltpu.VMEM((2, rows, width), bf16),
            pltpu.VMEM((2, rows, width), bf16),
            pltpu.VMEM((3, 2 * slots, ff // 2), bf16),
            pltpu.VMEM((2, 2 * slots, ff // 2), bf16),
            pltpu.VMEM((ff // 2, width), bf16),
            pltpu.VMEM((ff // 2, width), bf16),
            pltpu.VMEM((2, half, 2 * slots), bf16),
            pltpu.VMEM((2, 2 * slots, 1), f32),
            pltpu.VMEM((2, 2 * slots, width), bf16),
            pltpu.SemaphoreType.DMA((16,)),
            pltpu.SemaphoreType.DMA((80,)),
            pltpu.SemaphoreType.DMA((80,)),
        ],
        compiler_params=pltpu.CompilerParams(
            collective_id=0, has_side_effects=True, vmem_limit_bytes=60 * 1024 * 1024
        ),
    )(*operands)


def on_device(
    residual,
    pool_input,
    doc_ids,
    pool_map,
    pool_scale,
    out_weight,
    mix_gain,
    mix_shift,
    group_router,
    expert_router,
    expert_gate,
    expert_up,
    expert_down,
    routes,
    ffn_gain,
    ffn_shift,
):
    seq_rows = pool_input.shape[0]
    reach_rows = 15
    expert_count = lax.axis_size("sp")
    tp_count = lax.axis_size("tp")
    near = expert_count == 2 * group_size and tp_count == group_size
    near = near and residual.shape[0] == 2 * block and seq_rows == tp_count * residual.shape[0]
    if near:
        return near_layer(
            residual,
            pool_input,
            doc_ids,
            pool_map,
            pool_scale,
            out_weight,
            mix_gain,
            mix_shift,
            group_router,
            expert_router,
            expert_gate,
            expert_up,
            expert_down,
            routes,
            ffn_gain,
            ffn_shift,
        )
    window = jnp.left_shift(jnp.int32(2), lax.axis_index("tp"))
    first_row = lax.axis_index("sp") * seq_rows
    tail_values, tail_docs = from_behind(
        (pool_input[seq_rows - reach_rows :], doc_ids[seq_rows - reach_rows :]), "sp", 1
    )
    source = jnp.concatenate([tail_values, pool_input], axis=0).astype(jnp.float32)
    all_docs = jnp.concatenate([tail_docs, doc_ids], axis=0)
    positions = first_row - reach_rows + jnp.arange(seq_rows + reach_rows, dtype=jnp.int32)
    running = jnp.zeros((seq_rows, source.shape[1]), jnp.float32)
    weight_sum = jnp.zeros((seq_rows, 1), jnp.float32)
    for offset in range(reach_rows + 1):
        begin_row = reach_rows - offset
        earlier = source[begin_row : begin_row + seq_rows]
        keep_mask = (
            (all_docs[begin_row : begin_row + seq_rows] == doc_ids)
            & (positions[begin_row : begin_row + seq_rows] >= 0)
            & (offset < window)
        )
        same_doc = keep_mask.astype(jnp.float32)[:, None]
        running = running + same_doc * earlier
        weight_sum = weight_sum + same_doc
    pooled = (running / weight_sum - source[reach_rows:]).astype(jnp.bfloat16)
    mixed = (jnp.dot(pooled, pool_map[0], preferred_element_type=jnp.float32) * pool_scale).astype(
        jnp.bfloat16
    )
    row_count = seq_rows // tp_count
    blocks = mixed.reshape(tp_count, row_count, mixed.shape[1])
    branch = jnp.einsum(
        "abc,cd->abd",
        lax.all_to_all(blocks, "tp", split_axis=0, concat_axis=2, tiled=True),
        out_weight,
        preferred_element_type=jnp.float32,
    )[0]
    normed = layer_norm(
        skip_scale * residual.astype(jnp.float32) + branch, mix_gain, mix_shift
    ).astype(jnp.bfloat16)
    weight = route_weights(normed, routes, group_router, expert_router)
    half_most = row_count * routes.shape[1] // expert_count
    half_rows = row_count // 2
    routed_parts = []
    for piece_index in range(2):
        rows_here = slice(piece_index * half_rows, (piece_index + 1) * half_rows)
        outgoing, slot_index = fill_slots(
            normed[rows_here], routes[rows_here], half_most, expert_count
        )
        returned = lax.all_to_all(
            expert_ffn(
                lax.all_to_all(outgoing, "sp", split_axis=0, concat_axis=0, tiled=True),
                expert_gate,
                expert_up,
                expert_down,
            ),
            "sp",
            split_axis=0,
            concat_axis=0,
            tiled=True,
        )
        routed_parts.append(combine_rows(returned, slot_index, weight[rows_here]))
    routed = jnp.concatenate(routed_parts, axis=0)
    return layer_norm(skip_scale * normed.astype(jnp.float32) + routed, ffn_gain, ffn_shift).astype(
        jnp.bfloat16
    )


def solution(mesh):
    in_specs = (
        P(("sp", "tp"), None),
        P("sp", "tp"),
        P("sp"),
        P("tp", None, None),
        P("tp"),
        P(),
        P(),
        P(),
        P(),
        P(),
        P("sp", None, None),
        P("sp", None, None),
        P("sp", None, None),
        P(("sp", "tp"), None),
        P(),
        P(),
    )
    out_specs = P(("sp", "tp"), None)
    return jax.shard_map(
        on_device, mesh=mesh, in_specs=in_specs, out_specs=out_specs, check_vma=False
    )
```
